32 devices in a mesh: ep: 8 (over z, x), tp: 4 (over y, core).
Axes of the slice: x: 2, y: 2, z: 4, core: 2. Of those that a mesh axis runs over, the one named last changes fastest.
Arguments:
- tokens: bfloat16 [64, 2048], P(('ep', 'tp')), may hold values from -6 to 6
- cache_keys: bfloat16 [64, 1024, 256], P(('ep', 'tp')), may hold values from -360 to 360
- cache_values: bfloat16 [64, 1024, 256], P(('ep', 'tp')), may hold values from -6 to 6
- cache_gates: float32 [64, 2, 1024], P(('ep', 'tp')), may hold values from -256 to 0, as said below
- lengths: int32 [64], P(('ep', 'tp')), may hold values from 1 to 1024, 32768 in all
- routes: int32 [64, 4], P(('ep', 'tp')), may hold values from 0 to 7, all different within a row; in each aligned block of 2 rows (0 to 1, 2 to 3, ...) no two rows name the same one
- route_logits: float32 [64, 4], P(('ep', 'tp')), may hold values from -6 to 6
- attn_gain: float32 [2048], replicated, may hold values from 0.1 to 1.9
- w_query: bfloat16 [2048, 2048], P(None, 'tp'), may hold values from -0.125 to 0.125
- w_keyval: bfloat16 [2048, 512], P(None, 'tp'), may hold values from -0.125 to 0.125
- w_forget: bfloat16 [2048, 2], replicated, may hold values from -0.125 to 0.125
- forget_bias: float32 [2], replicated, may hold values from -1 to 3
- w_out: bfloat16 [2048, 2048], P(None, 'tp'), may hold values from -0.125 to 0.125
- mix_gain: float32 [2048], replicated, may hold values from 0.1 to 1.9
- ffn_gain: float32 [2048], replicated, may hold values from 0.1 to 1.9
- w_gate: bfloat16 [8, 2048, 2048], P('ep', None, 'tp'), may hold values from -0.125 to 0.125
- w_lin: bfloat16 [8, 2048, 2048], P('ep', None, 'tp'), may hold values from -0.125 to 0.125
- gate_bias: float32 [8, 2048], P('ep', 'tp'), may hold values from -12 to 12
- lin_bias: float32 [8, 2048], P('ep', 'tp'), may hold values from -12 to 12
- w_down: bfloat16 [8, 2048, 2048], P('ep', 'tp'), may hold values from -0.125 to 0.125
- post_gain: float32 [2048], replicated, may hold values from 0.1 to 1.9
Outputs:
- updated: bfloat16 [64, 2048], P(('ep', 'tp'))
- new_entries: bfloat16 [64, 512], P(('ep', 'tp'))
The draws below stay inside these ranges and needn't reach their ends.
Inputs may be any that keep to these rules, and one draw needn't show every extreme that they name: `cache_gates`: along the positions of each sequence and head the values never increase. The lengths of all sequences add up to 32768, and some sequence has exactly 1024. `routes`: each row names 4 different experts; among the rows of one device no expert is named twice; every expert is named by some row.
All inputs are finite; a program needn't handle non-finite values. No bound on the sum of `lengths` on one device may be relied on, other than what follows from the above.
Results may differ from the reference program's by a relative error of at most 0.014.
The reference program's roundings to bfloat16 on the way count: a program that leaves them out, or rounds other values in their place, can miss the bound.
Values may be sent and summed in bfloat16 or wider, within the bound.
No kernel may reach another device: no remote copies, remote signals or barrier semaphores. Data moves between devices by JAX's collectives and lax.ppermute only.
A program may use at most 64 MiB of HBM per device.

```python
import math
import jax
import jax.numpy as jnp
import numpy as np
from jax import lax

D = 2048
HEADS = 16
KVH = 2
HDIM = 128
FF = 2048
TOPK = 4
SEQ_DEV = 2
LEN = 1024
TOKENS = 64
EXPERTS = 8
N_TP = 4


def draw_cache_keys(key, part):
    first = jax.random.fold_in(jax.random.fold_in(key, 11), 0)
    values = jax.random.normal(first, (TOKENS, LEN, KVH * HDIM), jnp.float32)
    return jnp.clip(values, -360.0, 360.0).astype(jnp.bfloat16)


def draw_cache_gates(key, part):
    parts = jax.random.split(jax.random.fold_in(key, 23), 6)
    span = 32
    noise = jax.random.uniform(parts[0], (TOKENS, KVH, LEN), jnp.float32, 0.5, 1.5)
    blocks = jnp.exp(jax.random.uniform(parts[1], (TOKENS, 1, LEN // span), jnp.float32, -0.7, 0.7))
    blocks = jnp.repeat(blocks, span, axis=2)
    per_seq = jnp.exp(jax.random.uniform(parts[2], (TOKENS, 1, 1), jnp.float32, -0.7, 0.7))
    share = 0.5
    slow = jax.random.uniform(parts[3], (TOKENS, KVH, 1), jnp.float32) < share
    fast_rate = jnp.exp(jax.random.uniform(parts[4], (TOKENS, KVH, 1), jnp.float32, math.log(1.0 / 60.0), math.log(1.0 / 30.0)))
    slow_rate = jnp.exp(jax.random.uniform(parts[5], (TOKENS, KVH, 1), jnp.float32, -0.7, 0.0)) / LEN
    rate = jnp.where(slow, slow_rate, fast_rate)
    return jnp.cumsum(-rate * noise * blocks * per_seq, axis=2)


def block_levels(own_key, extent, cuts, smallest, largest):
    level, own = 1.0, jax.random.fold_in(own_key, 6)
    for axis_at, blocks in cuts:
        draws = jnp.exp(jax.random.uniform(jax.random.fold_in(own, axis_at), (blocks,), jnp.float32, smallest / len(cuts), largest / len(cuts)))
        level = level * jnp.repeat(draws, extent[axis_at] // blocks).reshape([-1 if axis == axis_at else 1 for axis in range(len(extent))])
    return level


def split_up(number_of, total, bound, lean):
    loads = [(1 << 20) // math.isqrt(grade ** lean) + 1 for grade in range(2, number_of + 1)]
    rest, counts = total - bound - (number_of - 1), [1] * (number_of - 1)
    while rest > 0:
        movable = [i for i in range(number_of - 1) if counts[i] < bound]
        whole, left = sum([loads[i] for i in movable]), rest
        for i in movable:
            addition = min(bound - counts[i], max(1, left * loads[i] // whole), rest)
            counts[i] = counts[i] + addition
            rest = rest - addition
    return np.array([bound] + counts)


def ragged(own_key, number_of, total, limit, skew):
    if number_of == 2:
        one = jax.random.randint(own_key, (), max(1, total - limit), min(limit, total - 1) + 1)
        return jnp.stack([one, total - one])
    sizes = jnp.asarray(split_up(number_of, total, limit, skew), jnp.int32)
    couples = (number_of - 1) // 2
    donor, receiver = sizes[1:1 + 2 * couples:2], sizes[2:2 + 2 * couples:2]
    slack = jnp.minimum(donor - 1, limit - receiver)
    moved = jax.random.randint(jax.random.fold_in(own_key, 1), (couples,), 0, 1 << 20) % (slack + 1)
    sizes = sizes.at[1:1 + 2 * couples:2].set(donor - moved).at[2:2 + 2 * couples:2].set(receiver + moved)
    return sizes[jax.random.permutation(jax.random.fold_in(own_key, 2), number_of)]


def routed_block(rng, own, number, rows, amount, top, reach, skew):
    ranking = jax.random.permutation(rng, amount)
    heavy_load, usual = load_shares(amount, rows * top, reach, skew, True), load_shares(amount, rows * top, reach, skew, False)
    places = jnp.arange(amount)

    def named(sizes, rotation):
        used = int((sizes > 0).sum())
        fixed = max(1, used // 4)
        passed = fixed + (places - fixed + rotation * (used - fixed)) % max(1, amount - fixed)
        return jnp.zeros((amount,), jnp.int32).at[ranking[jnp.where(places < fixed, places, passed)]].set(jnp.asarray(sizes, jnp.int32))

    sizes = jnp.where(number % 4 == 0, named(heavy_load, number // 4), named(usual, number - number // 4 - 1))
    mixed = jax.random.permutation(jax.random.fold_in(own, 3), amount)
    donor, sink = mixed[0:amount // 2 * 2:2], mixed[1:amount // 2 * 2:2]
    margin = jnp.minimum(sizes[donor] - 1, reach - sizes[sink]) // 2
    margin = jnp.where((donor == ranking[0]) | (sink == ranking[0]) | (sizes[sink] == 0), 0, jnp.maximum(margin, 0))
    passed = jax.random.randint(jax.random.fold_in(own, 4), (amount // 2,), 0, 1 << 20) % (margin + 1)
    sizes = sizes.at[donor].add(-passed).at[sink].add(passed)
    labels = jnp.searchsorted(jnp.cumsum(sizes), jnp.arange(rows * top), side="right").astype(jnp.int32)
    table = labels.reshape(top, rows).T
    table = table[jax.random.permutation(jax.random.fold_in(own, 1), rows)]
    rotation = jax.random.randint(jax.random.fold_in(own, 2), (rows, 1), 0, top)
    return jnp.take_along_axis(table, (jnp.arange(top)[None, :] + rotation) % top, axis=1)


def load_shares(amount, total, reach, skew, full):
    portions = [(1 << 20) // math.isqrt(grade ** skew) + 1 for grade in range(1, amount + 1)]
    largest = reach if full else min(reach, max(-(-total // amount), total * portions[0] // sum(portions)))
    least = 1 if total - largest >= amount - 1 else 0
    given, rest = [largest] + [least] * (amount - 1), total - largest - least * (amount - 1)
    while rest > 0:
        free = [i for i in range(1, amount) if given[i] < largest] or [i for i in range(1, amount) if given[i] < reach]
        whole, budget = sum([portions[i] for i in free]), rest
        for i in free:
            more = min(reach - given[i], max(1, budget * portions[i] // whole), rest)
            given[i] = given[i] + more
            rest = rest - more
    return np.array(given)


def gaussian(key, shape, deviation, reach, pieces=(), held_as=jnp.bfloat16):
    drawn = jax.random.normal(key, shape, jnp.float32) * deviation
    if len(pieces) > 0:
        drawn = block_levels(key, shape, pieces, -0.22, 0.18) * drawn
    return jnp.clip(drawn, min=-reach, max=reach).astype(held_as)


def setup_inputs(seed: int = 0) -> dict:
    splits = jax.random.split(jax.random.key(seed), 22)
    tokens = gaussian(splits[0], (TOKENS, D), 1.0, 6.0, ((0, 32),))
    cache_keys = draw_cache_keys(jax.random.fold_in(splits[21], 71), 0)
    cache_values = gaussian(splits[2], (TOKENS, LEN, KVH * HDIM), 1.0, 6.0, ((0, 32),))
    cache_gates = draw_cache_gates(jax.random.fold_in(splits[21], 71), 0)
    lengths = ragged(splits[4], TOKENS, TOKENS * LEN // 2, LEN, 2).astype(jnp.int32)
    routes_keys = jax.random.split(jax.random.fold_in(splits[5], 1), TOKENS // SEQ_DEV)
    routes_turns = jax.random.permutation(jax.random.fold_in(splits[5], 3), TOKENS // SEQ_DEV)
    routes = jax.vmap(lambda own, number: routed_block(jax.random.fold_in(splits[5], 2), own, number, SEQ_DEV, EXPERTS, TOPK, 1, 2))(routes_keys, routes_turns).reshape((TOKENS, TOPK))
    route_logits = gaussian(splits[6], (TOKENS, TOPK), 1.0, 6.0, ((0, 32),), jnp.float32)
    attn_gain = jnp.clip(1.0 + 0.18 * jax.random.normal(splits[7], (D,), jnp.float32), 0.1, 1.9)
    w_query = gaussian(splits[8], (D, HEADS * HDIM), D ** -0.5, 0.125, ((1, 4),))
    w_keyval = gaussian(splits[9], (D, 2 * KVH * HDIM), D ** -0.5, 0.125, ((1, 4),))
    w_forget = gaussian(splits[10], (D, KVH), D ** -0.5, 0.125)
    forget_bias = jnp.clip(jax.random.uniform(splits[11], (KVH,), jnp.float32, -1.0, 3.0), -1.0, 3.0)
    w_out = gaussian(splits[12], (HEADS * HDIM, D), (HEADS * HDIM) ** -0.5, 0.125, ((1, 4),))
    mix_gain = jnp.clip(1.0 + 0.18 * jax.random.normal(splits[13], (D,), jnp.float32), 0.1, 1.9)
    ffn_gain = jnp.clip(1.0 + 0.18 * jax.random.normal(splits[14], (D,), jnp.float32), 0.1, 1.9)
    w_gate = gaussian(splits[15], (EXPERTS, D, FF), D ** -0.5, 0.125, ((0, 8), (2, 4)))
    w_lin = gaussian(splits[16], (EXPERTS, D, FF), D ** -0.5, 0.125, ((0, 8), (2, 4)))
    gate_bias = gaussian(splits[17], (EXPERTS, FF), 3.0, 12.0, ((0, 8), (1, 4)), jnp.float32)
    lin_bias = gaussian(splits[18], (EXPERTS, FF), 3.0, 12.0, ((0, 8), (1, 4)), jnp.float32)
    w_down = gaussian(splits[19], (EXPERTS, FF, D), FF ** -0.5, 0.125, ((0, 8), (1, 4)))
    post_gain = jnp.clip(1.0 + 0.18 * jax.random.normal(splits[20], (D,), jnp.float32), 0.1, 1.9)
    return dict(tokens=tokens, cache_keys=cache_keys, cache_values=cache_values, cache_gates=cache_gates, lengths=lengths, routes=routes, route_logits=route_logits, attn_gain=attn_gain, w_query=w_query, w_keyval=w_keyval, w_forget=w_forget, forget_bias=forget_bias, w_out=w_out, mix_gain=mix_gain, ffn_gain=ffn_gain, w_gate=w_gate, w_lin=w_lin, gate_bias=gate_bias, lin_bias=lin_bias, w_down=w_down, post_gain=post_gain)


NORM_EPS = 1e-06
SWIGLU_ALPHA = 1.702
SWIGLU_LIMIT = 7.0
NEG_LARGE = -1e+30

def to_half(values):
    return lax.optimization_barrier(values.astype(jnp.bfloat16)).astype(jnp.float32)

def rms_scale(values, gain):
    values = values.astype(jnp.float32)
    return values * lax.rsqrt(lax.optimization_barrier(jnp.mean(values * values, axis=-1, keepdims=True)) + NORM_EPS) * gain.astype(jnp.float32)

def clamped_unit(gate, linear):
    gate = jnp.minimum(gate, SWIGLU_LIMIT)
    linear = jnp.clip(linear, -SWIGLU_LIMIT, SWIGLU_LIMIT)
    return gate * jax.nn.sigmoid(SWIGLU_ALPHA * gate) * (linear + 1.0)

def attend_one(args):
    query, fresh, keys, values, gates, length, forget = args
    group = HEADS // KVH
    q_four = query.reshape(KVH, group, HDIM).astype(jnp.float32)
    k_four = keys.reshape(LEN, KVH, HDIM).astype(jnp.float32)
    v_four = values.reshape(LEN, KVH, HDIM).astype(jnp.float32)
    new_key = fresh[:KVH * HDIM].reshape(KVH, HDIM).astype(jnp.float32)
    new_value = fresh[KVH * HDIM:].reshape(KVH, HDIM).astype(jnp.float32)
    place = jnp.arange(LEN, dtype=jnp.int32)
    last = lax.optimization_barrier(jnp.sum(jnp.where(place[None, :] == length - 1, gates, 0.0), axis=1))
    base = last + forget
    scale = HDIM ** (-0.5)
    scores = jnp.einsum('gqd,pgd->gqp', q_four, k_four) * scale + (base[:, None, None] - gates[:, None, :])
    live = place[None, None, :] < length
    masked = jnp.where(live, scores, NEG_LARGE)
    own = jnp.einsum('gqd,gd->gq', q_four, new_key) * scale
    top = jnp.maximum(lax.optimization_barrier(jnp.max(masked, axis=-1)), own)
    expo = jnp.where(live, jnp.exp(masked - top[..., None]), 0.0)
    own_expo = jnp.exp(own - top)
    total = lax.optimization_barrier(jnp.sum(expo, axis=-1)) + own_expo
    weights = to_half(expo / total[..., None])
    own_weight = to_half(own_expo / total)
    mixed = jnp.einsum('gqp,pgd->gqd', weights, v_four) + own_weight[..., None] * new_value[:, None, :]
    return mixed.reshape(HEADS * HDIM).astype(jnp.bfloat16)

def reference(tokens, cache_keys, cache_values, cache_gates, lengths, routes, route_logits, attn_gain, w_query, w_keyval, w_forget, forget_bias, w_out, mix_gain, ffn_gain, w_gate, w_lin, gate_bias, lin_bias, w_down, post_gain):
    normed = rms_scale(tokens, attn_gain).astype(jnp.bfloat16)
    query = jnp.dot(normed, w_query, preferred_element_type=jnp.float32).astype(jnp.bfloat16)
    fresh = jnp.dot(normed, w_keyval, preferred_element_type=jnp.float32).astype(jnp.bfloat16)
    forget = jax.nn.log_sigmoid(jnp.dot(normed, w_forget, preferred_element_type=jnp.float32) + forget_bias.astype(jnp.float32))
    mixed = lax.map(attend_one, (query, fresh, cache_keys, cache_values, cache_gates, lengths.astype(jnp.int32), forget))
    projected = jnp.dot(mixed, w_out, preferred_element_type=jnp.float32).astype(jnp.bfloat16)
    residual = tokens.astype(jnp.float32) + rms_scale(projected, mix_gain)
    expert_in = rms_scale(residual, ffn_gain).astype(jnp.bfloat16)
    hit = (routes[:, :, None] == jnp.arange(EXPERTS, dtype=jnp.int32)[None, None, :]).astype(jnp.float32)
    probs = jax.nn.softmax(route_logits.astype(jnp.float32), axis=-1)
    combine = lax.optimization_barrier(jnp.sum(probs[:, :, None] * hit, axis=1))

    def expert_step(total, items):
        gate_w, lin_w, gate_b, lin_b, down_w, share = items
        gate = jnp.dot(expert_in, gate_w, preferred_element_type=jnp.float32) + gate_b.astype(jnp.float32)
        linear = jnp.dot(expert_in, lin_w, preferred_element_type=jnp.float32) + lin_b.astype(jnp.float32)
        act = clamped_unit(gate, linear).astype(jnp.bfloat16)
        blocked = act.reshape(TOKENS, N_TP, FF // N_TP).astype(jnp.float32)
        down_blocks = down_w.reshape(N_TP, FF // N_TP, D).astype(jnp.float32)
        parts = to_half(jnp.einsum('tnf,nfd->ntd', blocked, down_blocks))
        expert_out = to_half(lax.optimization_barrier(jnp.sum(parts, axis=0)))
        return (total + share[:, None] * expert_out, None)
    moe, _ = lax.scan(expert_step, jnp.zeros((TOKENS, D), jnp.float32), (w_gate, w_lin, gate_bias, lin_bias, w_down, combine.T))
    updated = (residual + rms_scale(moe, post_gain)).astype(jnp.bfloat16)
    return (updated, fresh)
```

```python
import jax
import jax.numpy as jnp
from jax import lax
from jax.sharding import PartitionSpec as P

HEADS = 16
KVH = 2
HDIM = 128
LANES = 128

NORM_EPS = 1e-06
SWIGLU_ALPHA = 1.702
SWIGLU_LIMIT = 7.0
NEG_LARGE = -1e30


def rms_scale(values, gain):
    values = values.astype(jnp.float32)
    return values * lax.rsqrt(jnp.mean(values * values, axis=-1, keepdims=True) + NORM_EPS) * gain


def clamped_unit(gate, linear):
    gate = jnp.minimum(gate, SWIGLU_LIMIT)
    linear = jnp.clip(linear, -SWIGLU_LIMIT, SWIGLU_LIMIT)
    return gate * jax.nn.sigmoid(SWIGLU_ALPHA * gate) * (linear + 1.0)


def peers(size):
    assert size & (size - 1) == 0
    return [[(j, j ^ k) for j in range(size)] for k in range(1, size)]


def swap_all(pieces):
    perms = peers(lax.axis_size("tp"))
    return [pieces[0]] + [lax.ppermute(p, "tp", perm) for p, perm in zip(pieces[1:], perms)]


def project_in(near, attn_gain, w_query, w_keyval):
    rows = jnp.concatenate(near, axis=0)
    normed = rms_scale(rows, attn_gain).astype(jnp.bfloat16)
    both = jnp.concatenate(
        [
            jnp.dot(normed, w_query, preferred_element_type=jnp.float32),
            jnp.dot(normed, w_keyval, preferred_element_type=jnp.float32),
        ],
        axis=1,
    ).astype(jnp.bfloat16)
    seqs = near[0].shape[0]
    return [both[k * seqs : (k + 1) * seqs] for k in range(len(near))]


def attend(near, base, cache_keys, cache_values, cache_gates, lengths, hit, query_cols):
    seqs, span = cache_keys.shape[:2]
    groups = len(near)
    here = lax.axis_index("tp")
    stacked = jnp.stack(near, axis=0)[jnp.arange(groups) ^ here]
    owned = stacked.transpose(1, 0, 2)
    query = owned[:, :, :query_cols].reshape(seqs, HEADS * HDIM)
    fresh = owned[:, :, query_cols:].reshape(seqs, 2 * KVH * HDIM)
    q_four = query.reshape(seqs, KVH, HEADS // KVH, HDIM)
    new_key = fresh[:, : KVH * HDIM].reshape(seqs, KVH, HDIM)
    new_value = fresh[:, KVH * HDIM :].reshape(seqs, KVH, HDIM)
    place = lax.iota(jnp.int32, span)
    scale = HDIM ** (-0.5)
    own = jnp.einsum("sgqd,sgd->sgq", q_four, new_key, preferred_element_type=jnp.float32) * scale
    keys_four = cache_keys.reshape(seqs, span, KVH, HDIM)
    values_four = cache_values.reshape(seqs, span, KVH, HDIM)
    scores = jnp.einsum("sgqd,spgd->sgqp", q_four, keys_four, preferred_element_type=jnp.float32)
    scores = scores * scale + (base[:, :, None, None] - cache_gates[:, :, None, :])
    live = place[None, None, None, :] < lengths[:, None, None, None]
    masked = jnp.where(live, scores, NEG_LARGE)
    top = jnp.maximum(jnp.max(masked, axis=-1), own)
    expo = jnp.where(live, jnp.exp(masked - top[..., None]), 0.0)
    own_expo = jnp.exp(own - top)
    total = jnp.sum(expo, axis=-1) + own_expo
    weights = (expo / total[..., None]).astype(jnp.bfloat16)
    mixed = jnp.einsum("sgqp,spgd->sgqd", weights, values_four, preferred_element_type=jnp.float32)
    own_weight = (own_expo / total).astype(jnp.bfloat16)
    mixed = (
        mixed
        + own_weight.astype(jnp.float32)[..., None] * new_value.astype(jnp.float32)[:, :, None, :]
    )
    mixed = mixed.reshape(seqs, HEADS * HDIM).astype(jnp.bfloat16)
    return jnp.concatenate([mixed, hit.astype(jnp.bfloat16)], axis=1), fresh


def project_out(near_mixed, near_tokens, w_out, experts):
    groups = len(near_mixed)
    seqs, width = near_tokens[0].shape
    rows = jnp.concatenate(near_mixed, axis=0)
    mixed, hit = rows[:, :width], rows[:, width : width + experts]
    cols = w_out.shape[1]
    projected = jnp.dot(mixed, w_out, preferred_element_type=jnp.float32).astype(jnp.bfloat16)
    here = lax.axis_index("tp")
    tokens = lax.dynamic_slice_in_dim(
        jnp.concatenate(near_tokens, axis=0), here * cols, cols, axis=1
    )
    hit = hit.reshape(groups, seqs, experts) > 0.5
    out = []
    for part in (projected, tokens):
        part = part.reshape(groups, seqs, cols)
        picked = jnp.zeros((experts, groups, cols), jnp.bfloat16)
        for s in range(seqs):
            picked = jnp.where(hit[:, s].T[:, :, None], part[None, :, s], picked)
        out.append(picked)
    block = jnp.concatenate(out, axis=1)
    block = jnp.broadcast_to(block[:, None], (experts, groups, 2 * groups, cols))
    return block.reshape(experts * groups, 2 * groups, cols)


def run_expert(arrived, mix_gain, ffn_gain, w_gate, w_lin, gate_bias, lin_bias, w_down, experts):
    groups = arrived.shape[1] // 2
    cols = arrived.shape[2]
    width = groups * cols
    blocks = arrived.reshape(experts, groups, 2 * groups, cols)

    def rows_of(offset):
        rows = [
            jnp.concatenate([blocks[:, j, offset + (r ^ j)] for j in range(groups)], axis=1)
            for r in range(groups)
        ]
        return jnp.stack(rows, axis=1).reshape(experts * groups, width)

    projected, tokens = rows_of(0), rows_of(groups)
    residual = tokens.astype(jnp.float32) + rms_scale(projected, mix_gain)
    expert_in = rms_scale(residual, ffn_gain).astype(jnp.bfloat16)
    gate = jnp.dot(expert_in, w_gate, preferred_element_type=jnp.float32) + gate_bias
    linear = jnp.dot(expert_in, w_lin, preferred_element_type=jnp.float32) + lin_bias
    act = clamped_unit(gate, linear).astype(jnp.bfloat16)
    part = jnp.dot(act, w_down, preferred_element_type=jnp.float32).astype(jnp.bfloat16)
    here = lax.axis_index("tp")
    side = lax.dynamic_slice_in_dim(projected, here * cols, cols, axis=1)
    return jnp.concatenate([part, side], axis=1).reshape(experts * groups, -1, LANES)


def finish(returned, tokens, combine, first, mix_gain, post_gain, experts):
    seqs, width = tokens.shape
    count = returned.shape[0]
    groups = count // experts
    flat = returned.reshape(experts, groups, -1)
    parts = jnp.sum(flat[:, :, :width].astype(jnp.float32), axis=1)
    parts = parts.astype(jnp.bfloat16).astype(jnp.float32)
    side = flat[:, :, width:].reshape(experts, width)
    projected = side[first]
    residual = tokens.astype(jnp.float32) + rms_scale(projected, mix_gain)
    moe = jnp.einsum("se,ed->sd", combine, parts, precision=lax.Precision.HIGHEST)
    return (residual + rms_scale(moe, post_gain)).astype(jnp.bfloat16)


def per_device(
    tokens,
    cache_keys,
    cache_values,
    cache_gates,
    lengths,
    routes,
    route_logits,
    attn_gain,
    w_query,
    w_keyval,
    w_forget,
    forget_bias,
    w_out,
    mix_gain,
    ffn_gain,
    w_gate,
    w_lin,
    gate_bias,
    lin_bias,
    w_down,
    post_gain,
):
    groups = lax.axis_size("tp")
    experts = lax.axis_size("ep")
    both_axes = ("ep", "tp")

    near_tokens = swap_all([tokens] * groups)

    normed = rms_scale(tokens, attn_gain).astype(jnp.bfloat16)
    forget = jax.nn.log_sigmoid(
        jnp.dot(normed, w_forget, preferred_element_type=jnp.float32) + forget_bias
    )
    place = lax.iota(jnp.int32, cache_keys.shape[1])
    last = jnp.sum(
        jnp.where(place[None, None, :] == lengths[:, None, None] - 1, cache_gates, 0.0), axis=2
    )
    base = last + forget
    hit = (routes[:, :, None] == lax.iota(jnp.int32, experts)[None, None, :]).astype(jnp.float32)
    probs = jax.nn.softmax(route_logits, axis=-1)
    combine = jnp.sum(probs[:, :, None] * hit, axis=1)

    sent = project_in(near_tokens, attn_gain, w_query, w_keyval)
    near = swap_all(sent)
    mixed, fresh = attend(
        near,
        base,
        cache_keys,
        cache_values,
        cache_gates,
        lengths,
        jnp.sum(hit, axis=1),
        w_query.shape[1],
    )
    near_mixed = swap_all([mixed] * groups)
    outbound = project_out(near_mixed, near_tokens, w_out, experts)
    arrived = lax.all_to_all(outbound, both_axes, 0, 0, tiled=True)
    answers = run_expert(
        arrived,
        mix_gain,
        ffn_gain,
        w_gate[0],
        w_lin[0],
        gate_bias[0],
        lin_bias[0],
        w_down[0],
        experts,
    )
    returned = lax.all_to_all(answers, both_axes, 0, 0, tiled=True)
    updated = finish(returned, tokens, combine, routes[:, 0], mix_gain, post_gain, experts)
    return (updated, fresh)


def solution(mesh):
    in_specs = (
        P(("ep", "tp"), None),
        P(("ep", "tp"), None, None),
        P(("ep", "tp"), None, None),
        P(("ep", "tp"), None, None),
        P(("ep", "tp")),
        P(("ep", "tp"), None),
        P(("ep", "tp"), None),
        P(),
        P(None, "tp"),
        P(None, "tp"),
        P(),
        P(),
        P(None, "tp"),
        P(),
        P(),
        P("ep", None, "tp"),
        P("ep", None, "tp"),
        P("ep", "tp"),
        P("ep", "tp"),
        P("ep", "tp", None),
        P(),
    )
    out_specs = (P(("ep", "tp"), None), P(("ep", "tp"), None))
    return jax.shard_map(
        per_device, mesh=mesh, in_specs=in_specs, out_specs=out_specs, check_vma=False
    )
```

```python
import functools
import math

import jax
import jax.numpy as jnp
from jax import lax
from jax.experimental import pallas as pl
from jax.experimental.pallas import tpu as pltpu
from jax.sharding import PartitionSpec as P

HEADS = 16
KVH = 2
HDIM = 128
LANES = 128

NORM_EPS = 1e-06
SWIGLU_ALPHA = 1.702
SWIGLU_LIMIT = 7.0
NEG_LARGE = -1e30

LOAD_FLOPS = 50_000_000


F32 = jnp.float32
BF16 = jnp.bfloat16
VMEM = pltpu.VMEM
SMEM = pltpu.SMEM


def call(name, body, outs, args, smem=(), hbm=(), hbm_out=(), scratch=(), flops=0):
    spaces = [
        SMEM if i in smem else pl.ANY if i in hbm else VMEM for i in range(len(args))
    ]
    args = [
        pltpu.with_memory_space_constraint(a, VMEM)
        if space is VMEM
        else pltpu.with_memory_space_constraint(a, pltpu.HBM)
        if space is pl.ANY
        else a
        for a, space in zip(args, spaces)
    ]
    room = 4 << 20
    for entry in scratch:
        if isinstance(entry, tuple):
            room += 2 * math.prod(entry[0]) * jnp.dtype(entry[1]).itemsize
    return pl.pallas_call(
        body,
        out_shape=[
            jax.ShapeDtypeStruct(shape, dtype) if i in hbm_out else VMEM(shape, dtype)
            for i, (shape, dtype) in enumerate(outs)
        ],
        in_specs=[pl.BlockSpec(memory_space=space) for space in spaces],
        out_specs=[pl.BlockSpec(memory_space=VMEM) for _ in outs],
        scratch_shapes=[
            VMEM(*entry) if isinstance(entry, tuple) else entry for entry in scratch
        ],
        compiler_params=pltpu.CompilerParams(vmem_limit_bytes=room),
        cost_estimate=pl.CostEstimate(flops=flops, transcendentals=0, bytes_accessed=0),
        name=name,
    )(*args)


def load_body(*refs, pieces):
    count = len(pieces)
    sources, targets, sems = refs[:count], refs[count : 2 * count], refs[2 * count]
    copies = []
    for source, target, cuts in zip(sources, targets, pieces):
        size = source.shape[0] // cuts
        for c in range(cuts):
            part = pl.ds(c * size, size)
            copies.append(
                pltpu.make_async_copy(source.at[part], target.at[part], sems.at[len(copies)])
            )
    for copy in copies:
        copy.start()
    for copy in copies:
        copy.wait()


def load(name, arrays, pieces, flops):
    return call(
        name,
        functools.partial(load_body, pieces=pieces),
        [(a.shape, a.dtype) for a in arrays],
        arrays,
        hbm=range(len(arrays)),
        scratch=[pltpu.SemaphoreType.DMA((sum(pieces),))],
        flops=flops,
    )


def inverse_rms(values):
    return lax.rsqrt(jnp.mean(values * values, axis=-1, keepdims=True) + NORM_EPS)


def inverse_rms_all(values):
    return lax.rsqrt(jnp.mean(values * values, axis=(0, 1), keepdims=True) + NORM_EPS)


def clamped_unit(gate, linear):
    gate = jnp.minimum(gate, SWIGLU_LIMIT)
    linear = jnp.clip(linear, -SWIGLU_LIMIT, SWIGLU_LIMIT)
    return gate * jax.nn.sigmoid(SWIGLU_ALPHA * gate) * (linear + 1.0)


def peers(size):
    assert size & (size - 1) == 0
    return [[(j, j ^ k) for j in range(size)] for k in range(1, size)]


def swap_all(pieces):
    perms = peers(lax.axis_size("tp"))
    return [pieces[0]] + [lax.ppermute(p, "tp", perm) for p, perm in zip(pieces[1:], perms)]


def prepare_body(
    lengths, tokens, gain, w_forget, bias, gates, routes, logits, bias_out, hit_out, combine_out, pick_out, tok_out
):
    seqs, width = tokens.shape
    span = gates.shape[2]
    raw = tokens[...].astype(F32)
    normed = (raw * inverse_rms(raw) * gain[...]).astype(BF16).astype(F32)
    w_rows = w_forget[...].astype(F32)
    lane = lax.broadcasted_iota(jnp.int32, (KVH, span), 1)
    head = lax.broadcasted_iota(jnp.int32, (KVH, 1), 0)
    shift = jnp.zeros((KVH, 1), F32)
    for g in range(KVH):
        shift = jnp.where(head == g, bias[:, g : g + 1], shift)
    for s in range(seqs):
        logit = jnp.sum(normed[s : s + 1] * w_rows, axis=-1, keepdims=True) + shift
        forget = jnp.minimum(logit, 0.0) - jnp.log1p(jnp.exp(-jnp.abs(logit)))
        own_gates = gates[s]
        last = jnp.sum(jnp.where(lane == lengths[s] - 1, own_gates, 0.0), axis=-1, keepdims=True)
        bias_out[s] = jnp.where(lane < lengths[s], (last + forget) - own_gates, NEG_LARGE)
        for c in range(width // LANES):
            row = s * (width // LANES) + c
            tok_out[row : row + 1, :] = raw[s : s + 1, c * LANES : (c + 1) * LANES]
    chosen = routes[...]
    scores = logits[...]
    expo = jnp.exp(scores - jnp.max(scores, axis=-1, keepdims=True))
    probs = expo / jnp.sum(expo, axis=-1, keepdims=True)
    expert = lax.broadcasted_iota(jnp.int32, hit_out.shape, 1)
    hit = jnp.zeros(hit_out.shape, F32)
    combine = jnp.zeros(hit_out.shape, F32)
    for k in range(chosen.shape[1]):
        match = (chosen[:, k : k + 1] == expert).astype(F32)
        hit = hit + match
        combine = combine + probs[:, k : k + 1] * match
    pick_out[...] = (chosen[:, :1] == expert).astype(F32)
    hit_out[...] = hit
    combine_out[...] = combine


def project_in_body(*refs, groups):
    near, (gain, w_query, w_keyval) = refs[:groups], refs[groups : groups + 3]
    outs, rows = refs[groups + 3 : -1], refs[-1]
    seqs = near[0].shape[0]
    for k in range(groups):
        rows[k * seqs : (k + 1) * seqs, :] = near[k][...].astype(F32)
    raw = rows[...]
    normed = (raw * inverse_rms(raw) * gain[...]).astype(BF16)
    query = jnp.dot(normed, w_query[...], preferred_element_type=F32).astype(BF16)
    pair = jnp.dot(normed, w_keyval[...], preferred_element_type=F32).astype(BF16)
    cols = query.shape[1]
    for k in range(groups):
        outs[k][:, :cols] = query[k * seqs : (k + 1) * seqs]
        outs[k][:, cols:] = pair[k * seqs : (k + 1) * seqs]


def attend_body(*refs, groups, cols):
    near, (keys, values, bias, hit) = refs[:groups], refs[groups : groups + 4]
    mixed_out, fresh_out, pieces, q_rows, mixed_rows = refs[groups + 4 :]
    here = lax.axis_index("tp")
    seqs, width = near[0].shape
    pair = width - cols
    share = HEADS // KVH
    scale = HDIM ** (-0.5)
    for k in range(groups):
        pieces[here ^ k] = near[k][...].astype(F32)
    fresh = jnp.concatenate([pieces[c][:, cols:] for c in range(groups)], axis=1)
    fresh_out[...] = fresh.astype(BF16)
    q_rows[...] = jnp.zeros(q_rows.shape, F32)
    for s in range(seqs):
        for h in range(HEADS):
            c, at = h * HDIM // cols, h * HDIM % cols
            g = h // share
            q_rows[s * HEADS + h : s * HEADS + h + 1, g * HDIM : (g + 1) * HDIM] = pieces[
                c, s : s + 1, at : at + HDIM
            ]
    head = lax.broadcasted_iota(jnp.int32, (HEADS, 1), 0)
    for s in range(seqs):
        query = q_rows[s * HEADS : (s + 1) * HEADS, :]
        new_key = fresh[s : s + 1, : KVH * HDIM]
        new_value = fresh[s : s + 1, KVH * HDIM :]
        raw = lax.dot_general(
            query.astype(BF16), keys[s], (((1,), (1,)), ((), ())), preferred_element_type=F32
        )
        row_bias = bias[s, KVH - 1 : KVH, :]
        for g in range(KVH - 1):
            row_bias = jnp.where((head >= g * share) & (head < (g + 1) * share), bias[s, g : g + 1, :], row_bias)
        scores = raw * scale + row_bias
        own = jnp.sum(query * new_key, axis=-1, keepdims=True) * scale
        top = jnp.maximum(jnp.max(scores, axis=-1, keepdims=True), own)
        expo = jnp.exp(scores - top)
        own_expo = jnp.exp(own - top)
        total = 1.0 / (jnp.sum(expo, axis=-1, keepdims=True) + own_expo)
        weight = (expo * total).astype(BF16)
        own_weight = (own_expo * total).astype(BF16).astype(F32)
        mixed = jnp.dot(weight, values[s], preferred_element_type=F32) + own_weight * new_value
        for h in range(HEADS):
            g = h // share
            mixed_rows[s : s + 1, h * HDIM : (h + 1) * HDIM] = mixed[
                h : h + 1, g * HDIM : (g + 1) * HDIM
            ]
    full = HEADS * HDIM
    mixed_out[:, :full] = mixed_rows[:seqs, :].astype(BF16)
    mixed_out[:, full:] = hit[...].astype(BF16)


def project_out_body(*refs, groups, experts):
    near, tokens, w_out = refs[:groups], refs[groups : 2 * groups], refs[2 * groups]
    out, mixed_rows, parts, hits = refs[2 * groups + 1 :]
    here = lax.axis_index("tp")
    seqs = near[0].shape[0]
    width, cols = w_out.shape
    for k in range(groups):
        mixed_rows[k * seqs : (k + 1) * seqs, :] = near[k][:, :width].astype(F32)
        hit = near[k][:, width:].astype(F32)
        mine = tokens[k][:, pl.ds(pl.multiple_of(here * cols, LANES), cols)].astype(F32)
        for s in range(seqs):
            hits[s, k : k + 1, :] = hit[s : s + 1]
            hits[s, groups + k : groups + k + 1, :] = hit[s : s + 1]
            parts[s, groups + k : groups + k + 1, :] = mine[s : s + 1]
    projected = jnp.dot(mixed_rows[...].astype(BF16), w_out[...], preferred_element_type=F32)
    for k in range(groups):
        for s in range(seqs):
            parts[s, k : k + 1, :] = projected[k * seqs + s : k * seqs + s + 1]
    rows = [parts[s] for s in range(seqs)]
    marks = [hits[s] for s in range(seqs)]
    for e in range(experts):
        block = jnp.zeros(rows[0].shape, F32)
        for s in range(seqs):
            block = jnp.where(marks[s][:, e : e + 1] > 0.5, rows[s], block)
        block = block.astype(BF16)
        for j in range(groups):
            out[e * groups + j] = block


def expert_body(
    arrived, mix_gain, ffn_gain, w_gate, w_lin, gate_bias, lin_bias, w_down, out, wide, expert_in, answer,
    *, groups, experts, pitch
):
    here = lax.axis_index("tp")
    cols = arrived.shape[1]
    tall = 2 * groups
    step = groups * tall
    count = arrived.shape[0]
    width = groups * cols
    chunks = width // LANES
    per = cols // LANES
    for c in range(per):
        wide[c * count : (c + 1) * count, :] = arrived[:, c * LANES : (c + 1) * LANES].astype(F32)

    def pick(c, row):
        return wide[pl.ds(c * count + row, experts, stride=step), :]

    def rows_of(offset, r):
        return jnp.concatenate(
            [
                pick(c, j * tall + offset + (r ^ j)) for j in range(groups) for c in range(per)
            ],
            axis=1,
        )

    for r in range(groups):
        projected, tokens = rows_of(0, r), rows_of(groups, r)
        residual = tokens + projected * inverse_rms(projected) * mix_gain[...]
        normed = residual * inverse_rms(residual) * ffn_gain[...]
        expert_in[r * experts : (r + 1) * experts, :] = normed.astype(BF16)
        for c in range(per):
            answer[pl.ds(r * experts * pitch + chunks + c, experts, stride=pitch), :] = pick(
                c, here * tall + (here ^ r)
            )
    rows = expert_in[...]
    gate = jnp.dot(rows, w_gate[...], preferred_element_type=F32) + gate_bias[...]
    linear = jnp.dot(rows, w_lin[...], preferred_element_type=F32) + lin_bias[...]
    act = clamped_unit(gate, linear).astype(BF16)
    part = jnp.dot(act, w_down[...], preferred_element_type=F32)
    for c in range(chunks):
        answer[pl.ds(c, groups * experts, stride=pitch), :] = part[:, c * LANES : (c + 1) * LANES]
    used = out.shape[1]
    for r in range(groups):
        for e in range(experts):
            at = (r * experts + e) * pitch
            out[e * groups + r] = answer[at : at + used, :].astype(BF16)


def finish_body(
    returned, tokens, combine, pick, mix_gain, post_gain, out, rows, *, groups, experts
):
    seqs, width = out.shape
    chunks = width // LANES
    side = chunks // groups
    moe = [jnp.zeros((chunks, LANES), F32) for _ in range(seqs)]
    near = [[jnp.zeros((side, LANES), F32) for _ in range(groups)] for _ in range(seqs)]
    for e in range(experts):
        total = jnp.zeros((chunks, LANES), F32)
        picked = [pick[s : s + 1, e : e + 1] for s in range(seqs)]
        for j in range(groups):
            total = total + returned[e * groups + j, :chunks, :].astype(F32)
            slice_j = returned[e * groups + j, chunks:, :].astype(F32)
            for s in range(seqs):
                near[s][j] = near[s][j] + picked[s] * slice_j
        total = total.astype(BF16).astype(F32)
        for s in range(seqs):
            moe[s] = moe[s] + combine[s : s + 1, e : e + 1] * total
    for s in range(seqs):
        projected = jnp.concatenate(near[s], axis=0)
        own = tokens[s * chunks : (s + 1) * chunks, :]
        residual = own + projected * inverse_rms_all(projected) * mix_gain[...]
        updated = residual + moe[s] * inverse_rms_all(moe[s]) * post_gain[...]
        for c in range(chunks):
            rows[s : s + 1, c * LANES : (c + 1) * LANES] = updated[c : c + 1, :]
    out[...] = rows[:seqs, :].astype(BF16)


def per_device(
    tokens,
    cache_keys,
    cache_values,
    cache_gates,
    lengths,
    routes,
    route_logits,
    attn_gain,
    w_query,
    w_keyval,
    w_forget,
    forget_bias,
    w_out,
    mix_gain,
    ffn_gain,
    w_gate,
    w_lin,
    gate_bias,
    lin_bias,
    w_down,
    post_gain,
):
    groups = lax.axis_size("tp")
    experts = lax.axis_size("ep")
    both_axes = ("ep", "tp")
    seqs, width = tokens.shape
    span = cache_keys.shape[1]
    cols = w_query.shape[1]
    pair = w_keyval.shape[1]
    chunks = width // LANES
    marked = -(-experts // LANES) * LANES
    row = lambda gain: gain.reshape(1, width)
    block = lambda gain: gain.reshape(chunks, LANES)

    near_tokens = swap_all([tokens] * groups)
    w_query, w_keyval, keys, values, w_out = load(
        "load", [w_query, w_keyval, cache_keys, cache_values, w_out], (4, 1, 2, 2, 4), LOAD_FLOPS
    )
    bias, hit, combine, pick, own_tokens = call(
        "prepare",
        prepare_body,
        [((seqs, KVH, span), F32)] + [((seqs, marked), F32)] * 3 + [((seqs * chunks, LANES), F32)],
        [lengths, tokens, row(attn_gain), w_forget.T, forget_bias.reshape(1, KVH), cache_gates, routes, route_logits],
        smem=(0,),
    )
    sent = call(
        "project_in",
        functools.partial(project_in_body, groups=groups),
        [((seqs, cols + pair), BF16)] * groups,
        [*near_tokens, row(attn_gain), w_query, w_keyval],
        scratch=[((groups * seqs, width), F32)],
    )
    near = swap_all(sent)
    mixed, fresh = call(
        "attend",
        functools.partial(attend_body, groups=groups, cols=cols),
        [((seqs, width + marked), BF16), ((seqs, 2 * KVH * HDIM), BF16)],
        [*near, keys, values, bias, hit],
        scratch=[
            ((groups, seqs, cols + pair), F32),
            ((seqs * HEADS, KVH * HDIM), F32),
            ((max(seqs, 8), HEADS * HDIM), F32),
        ],
    )
    near_mixed = swap_all([mixed] * groups)
    (outbound,) = call(
        "project_out",
        functools.partial(project_out_body, groups=groups, experts=experts),
        [((experts * groups, 2 * groups, w_out.shape[1]), BF16)],
        [*near_mixed, *near_tokens, w_out],
        scratch=[
            ((groups * seqs, width), F32),
            ((seqs, 2 * groups, w_out.shape[1]), F32),
            ((seqs, 2 * groups, marked), F32),
        ],
    )
    arrived = lax.all_to_all(outbound, both_axes, 0, 0, tiled=True)
    used = chunks + chunks // groups
    pitch = -(-used // 8) * 8
    slots = experts * groups
    (answers,) = call(
        "expert",
        functools.partial(expert_body, groups=groups, experts=experts, pitch=pitch),
        [((slots, used, LANES), BF16)],
        [
            arrived.reshape(slots * 2 * groups, width // groups),
            row(mix_gain),
            row(ffn_gain),
            w_gate[0],
            w_lin[0],
            gate_bias,
            lin_bias,
            w_down[0],
        ],
        scratch=[
            ((slots * 2 * chunks, LANES), F32),
            ((slots, width), BF16),
            ((slots * pitch, LANES), F32),
        ],
    )
    returned = lax.all_to_all(answers, both_axes, 0, 0, tiled=True)
    (updated,) = call(
        "finish",
        functools.partial(finish_body, groups=groups, experts=experts),
        [((seqs, width), BF16)],
        [returned, own_tokens, combine, pick, block(mix_gain), block(post_gain)],
        hbm_out=(0,),
        scratch=[((max(seqs, 8), width), F32)],
    )
    return (updated, fresh)


def solution(mesh):
    in_specs = (
        P(("ep", "tp"), None),
        P(("ep", "tp"), None, None),
        P(("ep", "tp"), None, None),
        P(("ep", "tp"), None, None),
        P(("ep", "tp")),
        P(("ep", "tp"), None),
        P(("ep", "tp"), None),
        P(),
        P(None, "tp"),
        P(None, "tp"),
        P(),
        P(),
        P(None, "tp"),
        P(),
        P(),
        P("ep", None, "tp"),
        P("ep", None, "tp"),
        P("ep", "tp"),
        P("ep", "tp"),
        P("ep", "tp", None),
        P(),
    )
    out_specs = (P(("ep", "tp"), None), P(("ep", "tp"), None))
    return jax.shard_map(
        per_device, mesh=mesh, in_specs=in_specs, out_specs=out_specs, check_vma=False
    )
```

```python
import functools
import math

import jax
import jax.numpy as jnp
from jax import lax
from jax.experimental import pallas as pl
from jax.experimental.pallas import tpu as pltpu
from jax.sharding import PartitionSpec as P

HEADS = 16
KVH = 2
HDIM = 128
LANES = 128

NORM_EPS = 1e-06
SWIGLU_ALPHA = 1.702
SWIGLU_LIMIT = 7.0
NEG_LARGE = -1e30

LOAD_FLOPS = 50_000_000


F32 = jnp.float32
BF16 = jnp.bfloat16
VMEM = pltpu.VMEM
SMEM = pltpu.SMEM


def call(name, body, outs, args, smem=(), hbm=(), hbm_out=(), raw_out=(), scratch=(), flops=0):
    spaces = [
        SMEM if i in smem else pl.ANY if i in hbm else VMEM for i in range(len(args))
    ]
    args = [
        pltpu.with_memory_space_constraint(a, VMEM)
        if space is VMEM
        else pltpu.with_memory_space_constraint(a, pltpu.HBM)
        if space is pl.ANY
        else a
        for a, space in zip(args, spaces)
    ]
    room = 4 << 20
    for entry in scratch:
        if isinstance(entry, tuple):
            room += 2 * math.prod(entry[0]) * jnp.dtype(entry[1]).itemsize
    return pl.pallas_call(
        body,
        out_shape=[
            jax.ShapeDtypeStruct(shape, dtype) if i in (*hbm_out, *raw_out) else VMEM(shape, dtype)
            for i, (shape, dtype) in enumerate(outs)
        ],
        in_specs=[pl.BlockSpec(memory_space=space) for space in spaces],
        out_specs=[
            pl.BlockSpec(memory_space=pl.ANY if i in raw_out else VMEM) for i in range(len(outs))
        ],
        scratch_shapes=[
            VMEM(*entry) if isinstance(entry, tuple) else entry for entry in scratch
        ],
        compiler_params=pltpu.CompilerParams(vmem_limit_bytes=room),
        cost_estimate=pl.CostEstimate(flops=flops, transcendentals=0, bytes_accessed=0),
        name=name,
    )(*args)


def start_copies(sources, targets, sems, pieces):
    copies = []
    for source, target, cuts in zip(sources, targets, pieces):
        size = source.shape[0] // cuts
        for c in range(cuts):
            part = pl.ds(c * size, size)
            copies.append(
                pltpu.make_async_copy(source.at[part], target.at[part], sems.at[len(copies)])
            )
    for copy in copies:
        copy.start()
    return copies


def load_body(*refs, pieces):
    count = len(pieces)
    for copy in start_copies(refs[:count], refs[-count - 1 : -1], refs[-1], pieces):
        copy.wait()


def load(name, arrays, pieces, flops, after=(), out=()):
    return call(
        name,
        functools.partial(load_body, pieces=pieces),
        [(a.shape, a.dtype) for a in arrays],
        [*arrays, *after],
        hbm=[i for i in range(len(arrays)) if i not in out],
        raw_out=out,
        scratch=[pltpu.SemaphoreType.DMA((sum(pieces),))],
        flops=flops,
    )


def inverse_rms(values):
    return lax.rsqrt(jnp.mean(values * values, axis=-1, keepdims=True) + NORM_EPS)


def inverse_rms_all(values):
    return lax.rsqrt(jnp.mean(values * values, axis=(0, 1), keepdims=True) + NORM_EPS)


def clamped_unit(gate, linear):
    gate = jnp.minimum(gate, SWIGLU_LIMIT)
    linear = jnp.clip(linear, -SWIGLU_LIMIT, SWIGLU_LIMIT)
    return gate * jax.nn.sigmoid(SWIGLU_ALPHA * gate) * (linear + 1.0)


def peers(size):
    assert size & (size - 1) == 0
    return [[(j, j ^ k) for j in range(size)] for k in range(1, size)]


def swap_all(pieces):
    perms = peers(lax.axis_size("tp"))
    return [pieces[0]] + [lax.ppermute(p, "tp", perm) for p, perm in zip(pieces[1:], perms)]


def prepare_body(
    lengths, cache_values, tokens, gain, w_forget, bias, gates, routes, logits, after,
    values, bias_out, hit_out, combine_out, pick_out, tok_out, sems,
):
    del after
    copies = start_copies([cache_values], [values], sems, (2,))
    seqs, width = tokens.shape
    span = gates.shape[2]
    raw = tokens[...].astype(F32)
    normed = (raw * inverse_rms(raw) * gain[...]).astype(BF16).astype(F32)
    w_rows = w_forget[...].astype(F32)
    lane = lax.broadcasted_iota(jnp.int32, (KVH, span), 1)
    head = lax.broadcasted_iota(jnp.int32, (KVH, 1), 0)
    shift = jnp.zeros((KVH, 1), F32)
    for g in range(KVH):
        shift = jnp.where(head == g, bias[:, g : g + 1], shift)
    for s in range(seqs):
        logit = jnp.sum(normed[s : s + 1] * w_rows, axis=-1, keepdims=True) + shift
        forget = jnp.minimum(logit, 0.0) - jnp.log1p(jnp.exp(-jnp.abs(logit)))
        own_gates = gates[s]
        last = jnp.sum(jnp.where(lane == lengths[s] - 1, own_gates, 0.0), axis=-1, keepdims=True)
        bias_out[s] = jnp.where(lane < lengths[s], (last + forget) - own_gates, NEG_LARGE)
        for c in range(width // LANES):
            row = s * (width // LANES) + c
            tok_out[row : row + 1, :] = raw[s : s + 1, c * LANES : (c + 1) * LANES]
    chosen = routes[...]
    scores = logits[...]
    expo = jnp.exp(scores - jnp.max(scores, axis=-1, keepdims=True))
    probs = expo / jnp.sum(expo, axis=-1, keepdims=True)
    expert = lax.broadcasted_iota(jnp.int32, hit_out.shape, 1)
    hit = jnp.zeros(hit_out.shape, F32)
    combine = jnp.zeros(hit_out.shape, F32)
    for k in range(chosen.shape[1]):
        match = (chosen[:, k : k + 1] == expert).astype(F32)
        hit = hit + match
        combine = combine + probs[:, k : k + 1] * match
    pick_out[...] = (chosen[:, :1] == expert).astype(F32)
    hit_out[...] = hit
    combine_out[...] = combine
    for copy in copies:
        copy.wait()


def project_in_body(*refs, groups):
    near, (gain, w_query, w_keyval) = refs[:groups], refs[groups : groups + 3]
    outs, rows = refs[groups + 3 : -1], refs[-1]
    seqs = near[0].shape[0]
    for k in range(groups):
        rows[k * seqs : (k + 1) * seqs, :] = near[k][...].astype(F32)
    raw = rows[...]
    normed = (raw * inverse_rms(raw) * gain[...]).astype(BF16)
    query = jnp.dot(normed, w_query[...], preferred_element_type=F32).astype(BF16)
    pair = jnp.dot(normed, w_keyval[...], preferred_element_type=F32).astype(BF16)
    cols = query.shape[1]
    for k in range(groups):
        outs[k][:, :cols] = query[k * seqs : (k + 1) * seqs]
        outs[k][:, cols:] = pair[k * seqs : (k + 1) * seqs]


def attend_body(*refs, groups, cols):
    near, (keys, values, bias, hit) = refs[:groups], refs[groups : groups + 4]
    mixed_out, fresh_out, pieces, q_rows, mixed_rows = refs[groups + 4 :]
    here = lax.axis_index("tp")
    seqs, width = near[0].shape
    pair = width - cols
    share = HEADS // KVH
    scale = HDIM ** (-0.5)
    for k in range(groups):
        pieces[here ^ k] = near[k][...].astype(F32)
    fresh = jnp.concatenate([pieces[c][:, cols:] for c in range(groups)], axis=1)
    fresh_out[...] = fresh.astype(BF16)
    q_rows[...] = jnp.zeros(q_rows.shape, F32)
    for s in range(seqs):
        for h in range(HEADS):
            c, at = h * HDIM // cols, h * HDIM % cols
            g = h // share
            q_rows[s * HEADS + h : s * HEADS + h + 1, g * HDIM : (g + 1) * HDIM] = pieces[
                c, s : s + 1, at : at + HDIM
            ]
    head = lax.broadcasted_iota(jnp.int32, (HEADS, 1), 0)
    for s in range(seqs):
        query = q_rows[s * HEADS : (s + 1) * HEADS, :]
        new_key = fresh[s : s + 1, : KVH * HDIM]
        new_value = fresh[s : s + 1, KVH * HDIM :]
        raw = lax.dot_general(
            query.astype(BF16), keys[s], (((1,), (1,)), ((), ())), preferred_element_type=F32
        )
        row_bias = bias[s, KVH - 1 : KVH, :]
        for g in range(KVH - 1):
            row_bias = jnp.where((head >= g * share) & (head < (g + 1) * share), bias[s, g : g + 1, :], row_bias)
        scores = raw * scale + row_bias
        own = jnp.sum(query * new_key, axis=-1, keepdims=True) * scale
        top = jnp.maximum(jnp.max(scores, axis=-1, keepdims=True), own)
        expo = jnp.exp(scores - top)
        own_expo = jnp.exp(own - top)
        total = 1.0 / (jnp.sum(expo, axis=-1, keepdims=True) + own_expo)
        weight = (expo * total).astype(BF16)
        own_weight = (own_expo * total).astype(BF16).astype(F32)
        mixed = jnp.dot(weight, values[s], preferred_element_type=F32) + own_weight * new_value
        for h in range(HEADS):
            g = h // share
            mixed_rows[s : s + 1, h * HDIM : (h + 1) * HDIM] = mixed[
                h : h + 1, g * HDIM : (g + 1) * HDIM
            ]
    full = HEADS * HDIM
    mixed_out[:, :full] = mixed_rows[:seqs, :].astype(BF16)
    mixed_out[:, full:] = hit[...].astype(BF16)


def project_out_body(*refs, groups, experts, fold):
    near, tokens, w_out = refs[:groups], refs[groups : 2 * groups], refs[2 * groups]
    out, mixed_rows, parts, hits = refs[2 * groups + 1 :]
    here = lax.axis_index("tp")
    seqs = near[0].shape[0]
    width, cols = w_out.shape
    lanes = cols // fold

    def keep(which, k, rows):
        for s in range(seqs):
            for a in range(fold):
                parts[which * seqs + s, a * groups + k : a * groups + k + 1, :] = rows[
                    s : s + 1, a * lanes : (a + 1) * lanes
                ]

    for k in range(groups):
        mixed_rows[k * seqs : (k + 1) * seqs, :] = near[k][:, :width].astype(F32)
        hit = near[k][:, width:].astype(F32)
        for s in range(seqs):
            for a in range(fold):
                hits[s, a * groups + k : a * groups + k + 1, :] = hit[s : s + 1]
        keep(1, k, tokens[k][:, pl.ds(pl.multiple_of(here * cols, LANES), cols)].astype(F32))
    projected = jnp.dot(mixed_rows[...].astype(BF16), w_out[...], preferred_element_type=F32)
    for k in range(groups):
        keep(0, k, projected[k * seqs : (k + 1) * seqs])
    rows = [parts[n] for n in range(2 * seqs)]
    marks = [hits[s] for s in range(seqs)]
    for e in range(experts):
        on = [marks[s][:, e : e + 1] > 0.5 for s in range(seqs)]
        for which in range(2):
            block = jnp.zeros(rows[0].shape, F32)
            for s in range(seqs):
                block = jnp.where(on[s], rows[which * seqs + s], block)
            block = block.astype(BF16)
            for j in range(which, groups, 2):
                out[e * groups + j] = block


def expert_body(
    arrived, other, mix_gain, ffn_gain, w_gate, w_lin, gate_bias, lin_bias, w_down, out, wide, expert_in, answer,
    *, groups, experts, fold
):
    here = lax.axis_index("tp")
    count, lanes = arrived.shape
    tall = fold * groups
    step = groups * tall
    width = w_gate.shape[0]
    chunks = width // LANES
    side = chunks // groups
    per = lanes // LANES
    blocks, height = out.shape[1:3]
    pitch = blocks * 8
    parity = here & 1
    for c in range(per):
        for source, which in ((arrived, parity), (other, 1 - parity)):
            at = pl.multiple_of((which * per + c) * count, 8)
            wide[pl.ds(at, count), :] = source[:, c * LANES : (c + 1) * LANES].astype(F32)

    def pick(which, j, k, chunk):
        row = (which * per + chunk % per) * count + j * tall + chunk // per * groups + k
        return wide[pl.ds(row, experts, stride=step), :]

    def rows_of(which, r):
        return jnp.concatenate(
            [pick(which, j, r ^ j, chunk) for j in range(groups) for chunk in range(side)], axis=1
        )

    def spot(chunk):
        return chunk // height * 8 + chunk % height

    if blocks * height > chunks + side:
        answer[...] = jnp.zeros(answer.shape, F32)
    for r in range(groups):
        projected, tokens = rows_of(0, r), rows_of(1, r)
        residual = tokens + projected * inverse_rms(projected) * mix_gain[...]
        normed = residual * inverse_rms(residual) * ffn_gain[...]
        expert_in[r * experts : (r + 1) * experts, :] = normed.astype(BF16)
        for c in range(side):
            answer[pl.ds(r * experts * pitch + spot(chunks + c), experts, stride=pitch), :] = pick(
                0, here, here ^ r, c
            )
    rows = expert_in[...]
    gate = jnp.dot(rows, w_gate[...], preferred_element_type=F32) + gate_bias[...]
    linear = jnp.dot(rows, w_lin[...], preferred_element_type=F32) + lin_bias[...]
    act = clamped_unit(gate, linear).astype(BF16)
    part = jnp.dot(act, w_down[...], preferred_element_type=F32)
    for c in range(chunks):
        answer[pl.ds(spot(c), groups * experts, stride=pitch), :] = part[
            :, c * LANES : (c + 1) * LANES
        ]
    for r in range(groups):
        for e in range(experts):
            for b in range(blocks):
                at = (r * experts + e) * pitch + b * 8
                out[e * groups + r, b] = answer[at : at + height, :].astype(BF16)


def finish_body(
    returned, tokens, combine, pick, mix_gain, post_gain, out, rows, moe, near, *, groups, experts
):
    seqs, width = out.shape
    chunks = width // LANES
    side = chunks // groups
    height = returned.shape[2]
    tall = chunks // height
    zero = jnp.zeros((height, LANES), F32)
    sums = [[zero] * tall for _ in range(seqs)]
    own = [[zero] * groups for _ in range(seqs)]
    for e in range(experts):
        picked = [jnp.broadcast_to(pick[s : s + 1, e : e + 1], zero.shape) for s in range(seqs)]
        shares = [jnp.broadcast_to(combine[s : s + 1, e : e + 1], zero.shape) for s in range(seqs)]
        for b in range(tall):
            total = zero
            for j in range(groups):
                total = total + returned[e * groups + j, b].astype(F32)
            total = total.astype(BF16).astype(F32)
            for s in range(seqs):
                sums[s][b] = sums[s][b] + shares[s] * total
        for j in range(groups):
            part = returned[e * groups + j, tall].astype(F32)
            for s in range(seqs):
                own[s][j] = own[s][j] + picked[s] * part
    for s in range(seqs):
        for b in range(tall):
            moe[b * height : (b + 1) * height, :] = sums[s][b]
        for j in range(groups):
            near[j * side : (j + 1) * side, :] = own[s][j][:side]
        projected, mixture = near[...], moe[...]
        residual = (
            tokens[s * chunks : (s + 1) * chunks, :]
            + projected * inverse_rms_all(projected) * mix_gain[...]
        )
        updated = residual + mixture * inverse_rms_all(mixture) * post_gain[...]
        for c in range(chunks):
            rows[s : s + 1, c * LANES : (c + 1) * LANES] = updated[c : c + 1, :]
    out[...] = rows[:seqs, :].astype(BF16)


def per_device(
    tokens,
    cache_keys,
    cache_values,
    cache_gates,
    lengths,
    routes,
    route_logits,
    attn_gain,
    w_query,
    w_keyval,
    w_forget,
    forget_bias,
    w_out,
    mix_gain,
    ffn_gain,
    w_gate,
    w_lin,
    gate_bias,
    lin_bias,
    w_down,
    post_gain,
):
    groups = lax.axis_size("tp")
    experts = lax.axis_size("ep")
    both_axes = ("ep", "tp")
    seqs, width = tokens.shape
    span = cache_keys.shape[1]
    cols = w_query.shape[1]
    pair = w_keyval.shape[1]
    chunks = width // LANES
    slots = experts * groups
    out_cols = w_out.shape[1]
    fold = 2 if groups < 8 and out_cols % (2 * LANES) == 0 else 1
    marked = -(-experts // LANES) * LANES
    row = lambda gain: gain.reshape(1, width)
    block = lambda gain: gain.reshape(chunks, LANES)

    near_tokens = swap_all([tokens] * groups)
    w_query, w_keyval, keys = load(
        "load_in", [w_query, w_keyval, cache_keys], (2, 1, 2), LOAD_FLOPS
    )
    sent = call(
        "project_in",
        functools.partial(project_in_body, groups=groups),
        [((seqs, cols + pair), BF16)] * groups,
        [*near_tokens, row(attn_gain), w_query, w_keyval],
        scratch=[((groups * seqs, width), F32)],
    )
    near = swap_all(sent)
    values, bias, hit, combine, pick, own_tokens = call(
        "prepare",
        prepare_body,
        [
            (cache_values.shape, BF16),
            ((seqs, KVH, span), F32),
            ((seqs, marked), F32),
            ((seqs, marked), F32),
            ((seqs, marked), F32),
            ((seqs * chunks, LANES), F32),
        ],
        [
            lengths,
            cache_values,
            tokens,
            row(attn_gain),
            w_forget.T,
            forget_bias.reshape(1, KVH),
            cache_gates,
            routes,
            route_logits,
            sent[0],
        ],
        smem=(0,),
        hbm=(1,),
        scratch=[pltpu.SemaphoreType.DMA((2,))],
        flops=LOAD_FLOPS,
    )
    mixed, fresh = call(
        "attend",
        functools.partial(attend_body, groups=groups, cols=cols),
        [((seqs, width + marked), BF16), ((seqs, 2 * KVH * HDIM), BF16)],
        [*near, keys, values, bias, hit],
        scratch=[
            ((groups, seqs, cols + pair), F32),
            ((seqs * HEADS, KVH * HDIM), F32),
            ((max(seqs, 8), HEADS * HDIM), F32),
        ],
    )
    near_mixed = swap_all([mixed] * groups)
    w_out, fresh = load("load_out", [w_out, fresh], (2, 1), LOAD_FLOPS, [mixed], out=(1,))
    (outbound,) = call(
        "project_out",
        functools.partial(project_out_body, groups=groups, experts=experts, fold=fold),
        [((slots, fold * groups, out_cols // fold), BF16)],
        [*near_mixed, *near_tokens, w_out],
        scratch=[
            ((groups * seqs, width), F32),
            ((2 * seqs, fold * groups, out_cols // fold), F32),
            ((seqs, fold * groups, marked), F32),
        ],
    )
    arrived = lax.all_to_all(outbound, both_axes, 0, 0, tiled=True)
    arrived = arrived.reshape(slots * fold * groups, out_cols // fold)
    other = lax.ppermute(arrived, "tp", [(j, j ^ 1) for j in range(groups)])
    used = chunks + chunks // groups
    height = 4 if 1 <= used % 8 <= 4 else 8
    blocks = -(-used // height)
    (answers,) = call(
        "expert",
        functools.partial(expert_body, groups=groups, experts=experts, fold=fold),
        [((slots, blocks, height, LANES), BF16)],
        [
            arrived,
            other,
            row(mix_gain),
            row(ffn_gain),
            w_gate[0],
            w_lin[0],
            gate_bias,
            lin_bias,
            w_down[0],
        ],
        scratch=[
            ((2 * slots * chunks, LANES), F32),
            ((slots, width), BF16),
            ((slots * blocks * 8, LANES), F32),
        ],
    )
    returned = lax.all_to_all(answers, both_axes, 0, 0, tiled=True)
    (updated,) = call(
        "finish",
        functools.partial(finish_body, groups=groups, experts=experts),
        [((seqs, width), BF16)],
        [returned, own_tokens, combine, pick, block(mix_gain), block(post_gain)],
        hbm_out=(0,),
        scratch=[
            ((max(seqs, 8), width), F32),
            ((chunks, LANES), F32),
            ((chunks, LANES), F32),
        ],
    )
    return (updated, fresh)


def solution(mesh):
    in_specs = (
        P(("ep", "tp"), None),
        P(("ep", "tp"), None, None),
        P(("ep", "tp"), None, None),
        P(("ep", "tp"), None, None),
        P(("ep", "tp")),
        P(("ep", "tp"), None),
        P(("ep", "tp"), None),
        P(),
        P(None, "tp"),
        P(None, "tp"),
        P(),
        P(),
        P(None, "tp"),
        P(),
        P(),
        P("ep", None, "tp"),
        P("ep", None, "tp"),
        P("ep", "tp"),
        P("ep", "tp"),
        P("ep", "tp", None),
        P(),
    )
    out_specs = (P(("ep", "tp"), None), P(("ep", "tp"), None))
    return jax.shard_map(
        per_device, mesh=mesh, in_specs=in_specs, out_specs=out_specs, check_vma=False
    )
```

```python
import functools
import math

import jax
import jax.numpy as jnp
from jax import lax
from jax.experimental import pallas as pl
from jax.experimental.pallas import tpu as pltpu
from jax.sharding import PartitionSpec as P


HEADS = 16
KVH = 2
HDIM = 128
LANES = 128

NORM_EPS = 1e-06
SWIGLU_ALPHA = 1.702
SWIGLU_LIMIT = 7.0
NEG_LARGE = -1e30

LOAD_FLOPS = 50_000_000


F32 = jnp.float32
BF16 = jnp.bfloat16
VMEM = pltpu.VMEM
SMEM = pltpu.SMEM


def call(body, outs, args, smem=(), hbm=(), hbm_out=(), raw_out=(), scratch=(), flops=0):
    spaces = [
        SMEM if i in smem else pl.ANY if i in hbm else VMEM for i in range(len(args))
    ]
    args = [
        pltpu.with_memory_space_constraint(a, VMEM)
        if space is VMEM
        else pltpu.with_memory_space_constraint(a, pltpu.HBM)
        if space is pl.ANY
        else a
        for a, space in zip(args, spaces)
    ]
    room = 4 << 20
    for entry in scratch:
        if isinstance(entry, tuple):
            room += 2 * math.prod(entry[0]) * jnp.dtype(entry[1]).itemsize
    return pl.pallas_call(
        body,
        out_shape=[
            jax.ShapeDtypeStruct(shape, dtype) if i in (*hbm_out, *raw_out) else VMEM(shape, dtype)
            for i, (shape, dtype) in enumerate(outs)
        ],
        in_specs=[pl.BlockSpec(memory_space=space) for space in spaces],
        out_specs=[
            pl.BlockSpec(memory_space=pl.ANY if i in raw_out else VMEM) for i in range(len(outs))
        ],
        scratch_shapes=[
            VMEM(*entry) if isinstance(entry, tuple) else entry for entry in scratch
        ],
        compiler_params=pltpu.CompilerParams(vmem_limit_bytes=room),
        cost_estimate=pl.CostEstimate(flops=flops, transcendentals=0, bytes_accessed=0),
    )(*args)


def start_copies(sources, targets, sems, pieces):
    copies = []
    for source, target, cuts in zip(sources, targets, pieces):
        size = source.shape[0] // cuts
        for c in range(cuts):
            part = pl.ds(c * size, size)
            copies.append(
                pltpu.make_async_copy(source.at[part], target.at[part], sems.at[len(copies)])
            )
    for copy in copies:
        copy.start()
    return copies


def load_body(*refs, pieces):
    count = len(pieces)
    for copy in start_copies(refs[:count], refs[-count - 1 : -1], refs[-1], pieces):
        copy.wait()


def load(arrays, pieces, flops, after=(), out=()):
    return call(
        functools.partial(load_body, pieces=pieces),
        [(a.shape, a.dtype) for a in arrays],
        [*arrays, *after],
        hbm=[i for i in range(len(arrays)) if i not in out],
        raw_out=out,
        scratch=[pltpu.SemaphoreType.DMA((sum(pieces),))],
        flops=flops,
    )


def inverse_rms(values):
    return lax.rsqrt(jnp.mean(values * values, axis=-1, keepdims=True) + NORM_EPS)


def inverse_rms_all(values):
    return lax.rsqrt(jnp.mean(values * values, axis=(0, 1), keepdims=True) + NORM_EPS)


def clamped_unit(gate, linear):
    gate = jnp.minimum(gate, SWIGLU_LIMIT)
    linear = jnp.clip(linear, -SWIGLU_LIMIT, SWIGLU_LIMIT)
    return gate * jax.nn.sigmoid(SWIGLU_ALPHA * gate) * (linear + 1.0)


def peers(size):
    assert size & (size - 1) == 0
    return [[(j, j ^ k) for j in range(size)] for k in range(1, size)]


def swap_all(pieces):
    out = [pieces[0]]
    for k, perm in enumerate(peers(lax.axis_size("tp")), 1):
        out.append(lax.ppermute(pieces[k], "tp", perm))
    return out


def prepare_body(
    keys, cache_values, lengths, tokens, gain, w_forget, bias, gates, routes, logits, after,
    flipped, values, bias_out, hit_out, combine_out, pick_out, tok_out, sems,
):
    del after
    copies = start_copies([cache_values], [values], sems, (2,))
    for s in range(keys.shape[0]):
        flipped[s] = keys[s].T
    seqs, width = tokens.shape
    span = gates.shape[2]
    raw = tokens[...].astype(F32)
    normed = (raw * inverse_rms(raw) * gain[...]).astype(BF16).astype(F32)
    w_rows = w_forget[...].astype(F32)
    lane = lax.broadcasted_iota(jnp.int32, (KVH, span), 1)
    head = lax.broadcasted_iota(jnp.int32, (KVH, 1), 0)
    shift = jnp.zeros((KVH, 1), F32)
    for g in range(KVH):
        shift = jnp.where(head == g, bias[:, g : g + 1], shift)
    for s in range(seqs):
        logit = jnp.sum(normed[s : s + 1] * w_rows, axis=-1, keepdims=True) + shift
        forget = jnp.minimum(logit, 0.0) - jnp.log1p(jnp.exp(-jnp.abs(logit)))
        own_gates = gates[s]
        live = lengths[:, s : s + 1]
        last = jnp.sum(jnp.where(lane == live - 1, own_gates, 0.0), axis=-1, keepdims=True)
        bias_out[s] = jnp.where(lane < live, (last + forget) - own_gates, NEG_LARGE)
        for c in range(width // LANES):
            row = s * (width // LANES) + c
            tok_out[row : row + 1, :] = raw[s : s + 1, c * LANES : (c + 1) * LANES]
    chosen = routes[...]
    scores = logits[...]
    expo = jnp.exp(scores - jnp.max(scores, axis=-1, keepdims=True))
    probs = expo / jnp.sum(expo, axis=-1, keepdims=True)
    expert = lax.broadcasted_iota(jnp.int32, hit_out.shape, 1)
    hit = jnp.zeros(hit_out.shape, F32)
    combine = jnp.zeros(hit_out.shape, F32)
    for k in range(chosen.shape[1]):
        match = (chosen[:, k : k + 1] == expert).astype(F32)
        hit = hit + match
        combine = combine + probs[:, k : k + 1] * match
    pick_out[...] = (chosen[:, :1] == expert).astype(F32)
    hit_out[...] = hit
    combine_out[...] = combine
    for copy in copies:
        copy.wait()


def project_in_body(*refs, groups):
    near, (gain, w_query, w_keyval) = refs[:groups], refs[groups : groups + 3]
    outs, rows = refs[groups + 3 : -1], refs[-1]
    seqs = near[0].shape[0]
    for k in range(groups):
        rows[k * seqs : (k + 1) * seqs, :] = near[k][...].astype(F32)
    raw = rows[...]
    normed = (raw * inverse_rms(raw) * gain[...]).astype(BF16)
    query = jnp.dot(normed, w_query[...], preferred_element_type=F32).astype(BF16)
    pair = jnp.dot(normed, w_keyval[...], preferred_element_type=F32).astype(BF16)
    cols = query.shape[1]
    for k in range(groups):
        outs[k][:, :cols] = query[k * seqs : (k + 1) * seqs]
        outs[k][:, cols:] = pair[k * seqs : (k + 1) * seqs]


def attend_body(*refs, groups, cols):
    near, (keys, values, bias, hit) = refs[:groups], refs[groups : groups + 4]
    mixed_out, fresh_out, pieces, q_rows, mixed_rows = refs[groups + 4 :]
    here = lax.axis_index("tp")
    seqs, _ = near[0].shape
    share = HEADS // KVH
    scale = HDIM ** (-0.5)
    for k in range(groups):
        pieces[here ^ k] = near[k][...].astype(F32)
    fresh = jnp.concatenate([pieces[c][:, cols:] for c in range(groups)], axis=1)
    fresh_out[...] = fresh.astype(BF16)
    q_rows[...] = jnp.zeros(q_rows.shape, F32)
    for s in range(seqs):
        for h in range(HEADS):
            c, at = h * HDIM // cols, h * HDIM % cols
            g = h // share
            q_rows[s * HEADS + h : s * HEADS + h + 1, g * HDIM : (g + 1) * HDIM] = pieces[
                c, s : s + 1, at : at + HDIM
            ]
    head = lax.broadcasted_iota(jnp.int32, (HEADS, 1), 0)
    for s in range(seqs):
        query = q_rows[s * HEADS : (s + 1) * HEADS, :]
        new_key = fresh[s : s + 1, : KVH * HDIM]
        new_value = fresh[s : s + 1, KVH * HDIM :]
        raw = jnp.dot(query.astype(BF16), keys[s], preferred_element_type=F32)
        row_bias = bias[s, KVH - 1 : KVH, :]
        for g in range(KVH - 1):
            row_bias = jnp.where((head >= g * share) & (head < (g + 1) * share), bias[s, g : g + 1, :], row_bias)
        scores = raw * scale + row_bias
        own = jnp.sum(query * new_key, axis=-1, keepdims=True) * scale
        top = jnp.maximum(jnp.max(scores, axis=-1, keepdims=True), own)
        expo = jnp.exp(scores - top)
        own_expo = jnp.exp(own - top)
        total = 1.0 / (jnp.sum(expo, axis=-1, keepdims=True) + own_expo)
        weight = (expo * total).astype(BF16)
        own_weight = (own_expo * total).astype(BF16).astype(F32)
        mixed = jnp.dot(weight, values[s], preferred_element_type=F32) + own_weight * new_value
        for h in range(HEADS):
            g = h // share
            mixed_rows[s : s + 1, h * HDIM : (h + 1) * HDIM] = mixed[
                h : h + 1, g * HDIM : (g + 1) * HDIM
            ]
    full = HEADS * HDIM
    mixed_out[:, :full] = mixed_rows[:seqs, :].astype(BF16)
    mixed_out[:, full:] = hit[...].astype(BF16)


def project_out_body(*refs, groups, experts, fold):
    near, tokens, w_out = refs[:groups], refs[groups : 2 * groups], refs[2 * groups]
    out, mixed_rows, parts, hits = refs[2 * groups + 1 :]
    here = lax.axis_index("tp")
    seqs = near[0].shape[0]
    width, cols = w_out.shape
    lanes = cols // fold

    def keep(which, k, rows):
        for s in range(seqs):
            for a in range(fold):
                parts[which * seqs + s, pl.ds(a * groups + (here ^ k), 1), :] = rows[
                    s : s + 1, a * lanes : (a + 1) * lanes
                ]

    for k in range(groups):
        mixed_rows[k * seqs : (k + 1) * seqs, :] = near[k][:, :width].astype(F32)
        hit = near[k][:, width:].astype(F32)
        for s in range(seqs):
            for a in range(fold):
                hits[s, pl.ds(a * groups + (here ^ k), 1), :] = hit[s : s + 1]
        keep(1, k, tokens[k][:, pl.ds(pl.multiple_of(here * cols, LANES), cols)].astype(F32))
    projected = jnp.dot(mixed_rows[...].astype(BF16), w_out[...], preferred_element_type=F32)
    for k in range(groups):
        keep(0, k, projected[k * seqs : (k + 1) * seqs])
    rows = [parts[n] for n in range(2 * seqs)]
    marks = [hits[s] for s in range(seqs)]
    for e in range(experts):
        on = [marks[s][:, e : e + 1] > 0.5 for s in range(seqs)]
        for which in range(2):
            block = jnp.zeros(rows[0].shape, F32)
            for s in range(seqs):
                block = jnp.where(on[s], rows[which * seqs + s], block)
            block = block.astype(BF16)
            for j in range(which, groups, 2):
                out[e * groups + j] = block


def expert_body(
    arrived, other, mix_gain, ffn_gain, w_gate, w_lin, gate_bias, lin_bias, w_down, out, expert_in, answer,
    *, groups, experts, fold
):
    here = lax.axis_index("tp")
    lanes = arrived.shape[1]
    tall = fold * groups
    width = w_gate.shape[0]
    chunks = width // LANES
    side = chunks // groups
    per = lanes // LANES
    blocks, height = out.shape[1:3]
    pitch = blocks * 8
    even = (here & 1) == 0

    def tile(slot, c):
        at = slot * tall
        if not isinstance(slot, int):
            at = pl.multiple_of(at, 8)
        spot = (pl.ds(at, tall), pl.ds(c * LANES, LANES))
        mine, theirs = arrived[spot].astype(F32), other[spot].astype(F32)
        return jnp.where(even, mine, theirs), jnp.where(even, theirs, mine)

    def spot(chunk):
        return chunk // height * 8 + chunk % height

    if blocks * height > chunks + side:
        answer[...] = jnp.zeros(answer.shape, F32)
    span = max(8 // groups, 1)
    for first in range(0, experts, span):
        near = range(first, first + span)
        projected, tokens = [], []
        for j in range(groups):
            tiles = [[tile(i * groups + j, c) for i in near] for c in range(per)]
            for a in range(fold):
                for c in range(per):
                    rows = [
                        [pair[n][a * groups : (a + 1) * groups] for pair in tiles[c]] for n in range(2)
                    ]
                    projected.append(jnp.concatenate(rows[0], axis=0))
                    tokens.append(jnp.concatenate(rows[1], axis=0))
        projected = jnp.concatenate(projected, axis=1)
        tokens = jnp.concatenate(tokens, axis=1)
        residual = tokens + projected * inverse_rms(projected) * mix_gain[...]
        normed = residual * inverse_rms(residual) * ffn_gain[...]
        at, count = first * groups, span * groups
        expert_in[at : at + count, :] = normed.astype(BF16)
        for c in range(per):
            tiles = [tile(i * groups + here, c)[0] for i in near]
            for a in range(fold):
                answer[pl.ds(at * pitch + spot(chunks + a * per + c), count, stride=pitch), :] = (
                    jnp.concatenate([t[a * groups : (a + 1) * groups] for t in tiles], axis=0)
                )
    rows = expert_in[...]
    gate = jnp.dot(rows, w_gate[...], preferred_element_type=F32) + gate_bias[...]
    linear = jnp.dot(rows, w_lin[...], preferred_element_type=F32) + lin_bias[...]
    act = clamped_unit(gate, linear).astype(BF16)
    part = jnp.dot(act, w_down[...], preferred_element_type=F32)
    for c in range(chunks):
        answer[pl.ds(spot(c), groups * experts, stride=pitch), :] = part[
            :, c * LANES : (c + 1) * LANES
        ]
    for slot in range(groups * experts):
        for b in range(blocks):
            at = slot * pitch + b * 8
            out[slot, b] = answer[at : at + height, :].astype(BF16)


def finish_body(
    returned, tokens, combine, pick, mix_gain, post_gain, out, rows, moe, near, *, groups, experts
):
    seqs, width = out.shape
    chunks = width // LANES
    side = chunks // groups
    height = returned.shape[2]
    tall = chunks // height
    zero = jnp.zeros((height, LANES), F32)
    sums = [[zero] * tall for _ in range(seqs)]
    own = [[zero] * groups for _ in range(seqs)]
    for e in range(experts):
        picked = [jnp.broadcast_to(pick[s : s + 1, e : e + 1], zero.shape) for s in range(seqs)]
        shares = [jnp.broadcast_to(combine[s : s + 1, e : e + 1], zero.shape) for s in range(seqs)]
        for b in range(tall):
            total = zero
            for j in range(groups):
                total = total + returned[e * groups + j, b].astype(F32)
            total = total.astype(BF16).astype(F32)
            for s in range(seqs):
                sums[s][b] = sums[s][b] + shares[s] * total
        for j in range(groups):
            part = returned[e * groups + j, tall].astype(F32)
            for s in range(seqs):
                own[s][j] = own[s][j] + picked[s] * part
    for s in range(seqs):
        for b in range(tall):
            moe[b * height : (b + 1) * height, :] = sums[s][b]
        for j in range(groups):
            near[j * side : (j + 1) * side, :] = own[s][j][:side]
        projected, mixture = near[...], moe[...]
        residual = (
            tokens[s * chunks : (s + 1) * chunks, :]
            + projected * inverse_rms_all(projected) * mix_gain[...]
        )
        updated = residual + mixture * inverse_rms_all(mixture) * post_gain[...]
        for c in range(chunks):
            rows[s : s + 1, c * LANES : (c + 1) * LANES] = updated[c : c + 1, :]
    out[...] = rows[:seqs, :].astype(BF16)


def layer(
    tokens,
    cache_keys,
    cache_values,
    cache_gates,
    lengths,
    routes,
    route_logits,
    attn_gain,
    w_query,
    w_keyval,
    w_forget,
    forget_bias,
    w_out,
    mix_gain,
    ffn_gain,
    w_gate,
    w_lin,
    gate_bias,
    lin_bias,
    w_down,
    post_gain,
):
    groups = lax.axis_size("tp")
    experts = lax.axis_size("ep")
    both_axes = ("ep", "tp")
    seqs, width = tokens.shape
    span = cache_keys.shape[1]
    cols = w_query.shape[1]
    pair = w_keyval.shape[1]
    chunks = width // LANES
    slots = experts * groups
    out_cols = w_out.shape[1]
    fold = 2 if groups < 8 and out_cols % (2 * LANES) == 0 else 1
    marked = -(-experts // LANES) * LANES
    row = lambda gain: gain.reshape(1, width)
    block = lambda gain: gain.reshape(chunks, LANES)

    near_tokens = swap_all([tokens] * groups)
    w_query, w_keyval, keys = load([w_query, w_keyval, cache_keys], (2, 1, 2), LOAD_FLOPS)
    sent = call(
        functools.partial(project_in_body, groups=groups),
        [((seqs, cols + pair), BF16)] * groups,
        [*near_tokens, row(attn_gain), w_query, w_keyval],
        scratch=[((groups * seqs, width), F32)],
    )
    near = swap_all(sent)
    keys, values, bias, hit, combine, pick, own_tokens = call(
        prepare_body,
        [
            ((seqs, KVH * HDIM, span), BF16),
            (cache_values.shape, BF16),
            ((seqs, KVH, span), F32),
            ((seqs, marked), F32),
            ((seqs, marked), F32),
            ((seqs, marked), F32),
            ((seqs * chunks, LANES), F32),
        ],
        [
            keys,
            cache_values,
            lengths.reshape(1, seqs),
            tokens,
            row(attn_gain),
            w_forget.T,
            forget_bias.reshape(1, KVH),
            cache_gates,
            routes,
            route_logits,
            sent[0],
        ],
        hbm=(1,),
        scratch=[pltpu.SemaphoreType.DMA((2,))],
        flops=LOAD_FLOPS,
    )
    mixed, fresh = call(
        functools.partial(attend_body, groups=groups, cols=cols),
        [((seqs, width + marked), BF16), ((seqs, 2 * KVH * HDIM), BF16)],
        [*near, keys, values, bias, hit],
        scratch=[
            ((groups, seqs, cols + pair), F32),
            ((seqs * HEADS, KVH * HDIM), F32),
            ((max(seqs, 8), HEADS * HDIM), F32),
        ],
    )
    near_mixed = swap_all([mixed] * groups)
    w_out, fresh = load([w_out, fresh], (2, 1), LOAD_FLOPS, [mixed], out=(1,))
    (outbound,) = call(
        functools.partial(project_out_body, groups=groups, experts=experts, fold=fold),
        [((slots, fold * groups, out_cols // fold), BF16)],
        [*near_mixed, *near_tokens, w_out],
        scratch=[
            ((groups * seqs, width), F32),
            ((2 * seqs, fold * groups, out_cols // fold), F32),
            ((seqs, fold * groups, marked), F32),
        ],
    )
    arrived = lax.all_to_all(outbound, both_axes, 0, 0, tiled=True)
    arrived = arrived.reshape(slots * fold * groups, out_cols // fold)
    other = lax.ppermute(arrived, "tp", [(j, j ^ 1) for j in range(groups)])
    used = chunks + chunks // groups
    height = 4 if 1 <= used % 8 <= 4 else 8
    blocks = -(-used // height)
    (answers,) = call(
        functools.partial(expert_body, groups=groups, experts=experts, fold=fold),
        [((slots, blocks, height, LANES), BF16)],
        [
            arrived,
            other,
            row(mix_gain),
            row(ffn_gain),
            w_gate[0],
            w_lin[0],
            gate_bias,
            lin_bias,
            w_down[0],
        ],
        scratch=[
            ((slots, width), BF16),
            ((slots * blocks * 8, LANES), F32),
        ],
    )
    returned = lax.all_to_all(answers, both_axes, 0, 0, tiled=True)
    (updated,) = call(
        functools.partial(finish_body, groups=groups, experts=experts),
        [((seqs, width), BF16)],
        [returned, own_tokens, combine, pick, block(mix_gain), block(post_gain)],
        hbm_out=(0,),
        scratch=[
            ((max(seqs, 8), width), F32),
            ((chunks, LANES), F32),
            ((chunks, LANES), F32),
        ],
    )
    return (updated, fresh)


def solution(mesh):
    in_specs = (
        P(("ep", "tp"), None),
        P(("ep", "tp"), None, None),
        P(("ep", "tp"), None, None),
        P(("ep", "tp"), None, None),
        P(("ep", "tp")),
        P(("ep", "tp"), None),
        P(("ep", "tp"), None),
        P(),
        P(None, "tp"),
        P(None, "tp"),
        P(),
        P(),
        P(None, "tp"),
        P(),
        P(),
        P("ep", None, "tp"),
        P("ep", None, "tp"),
        P("ep", "tp"),
        P("ep", "tp"),
        P("ep", "tp", None),
        P(),
    )
    out_specs = (P(("ep", "tp"), None), P(("ep", "tp"), None))
    return jax.shard_map(layer, mesh=mesh, in_specs=in_specs, out_specs=out_specs, check_vma=False)
```

```python
import functools
import math

import jax
import jax.numpy as jnp
from jax import lax
from jax.experimental import pallas as pl
from jax.experimental.pallas import tpu as pltpu
from jax.sharding import PartitionSpec as P


HEADS = 16
KVH = 2
HDIM = 128
LANES = 128

NORM_EPS = 1e-06
SWIGLU_ALPHA = 1.702
SWIGLU_LIMIT = 7.0
NEG_LARGE = -1e30

LOAD_FLOPS = 50_000_000


F32 = jnp.float32
BF16 = jnp.bfloat16
VMEM = pltpu.VMEM
SMEM = pltpu.SMEM


def call(body, outs, args, smem=(), hbm=(), hbm_out=(), raw_out=(), scratch=(), flops=0):
    spaces = [
        SMEM if i in smem else pl.ANY if i in hbm else VMEM for i in range(len(args))
    ]
    args = [
        pltpu.with_memory_space_constraint(a, VMEM)
        if space is VMEM
        else pltpu.with_memory_space_constraint(a, pltpu.HBM)
        if space is pl.ANY
        else a
        for a, space in zip(args, spaces)
    ]
    room = 4 << 20
    for entry in scratch:
        if isinstance(entry, tuple):
            room += 2 * math.prod(entry[0]) * jnp.dtype(entry[1]).itemsize
    return pl.pallas_call(
        body,
        out_shape=[
            jax.ShapeDtypeStruct(shape, dtype) if i in (*hbm_out, *raw_out) else VMEM(shape, dtype)
            for i, (shape, dtype) in enumerate(outs)
        ],
        in_specs=[pl.BlockSpec(memory_space=space) for space in spaces],
        out_specs=[
            pl.BlockSpec(memory_space=pl.ANY if i in raw_out else VMEM) for i in range(len(outs))
        ],
        scratch_shapes=[
            VMEM(*entry) if isinstance(entry, tuple) else entry for entry in scratch
        ],
        compiler_params=pltpu.CompilerParams(vmem_limit_bytes=room),
        cost_estimate=pl.CostEstimate(flops=flops, transcendentals=0, bytes_accessed=0),
    )(*args)


def start_copies(sources, targets, sems, pieces):
    copies = []
    for source, target, cuts in zip(sources, targets, pieces):
        size = source.shape[0] // cuts
        for c in range(cuts):
            part = pl.ds(c * size, size)
            copies.append(
                pltpu.make_async_copy(source.at[part], target.at[part], sems.at[len(copies)])
            )
    for copy in copies:
        copy.start()
    return copies


def load_body(*refs, pieces):
    count = len(pieces)
    for copy in start_copies(refs[:count], refs[-count - 1 : -1], refs[-1], pieces):
        copy.wait()


def load(arrays, pieces, flops, after=(), out=()):
    return call(
        functools.partial(load_body, pieces=pieces),
        [(a.shape, a.dtype) for a in arrays],
        [*arrays, *after],
        hbm=[i for i in range(len(arrays)) if i not in out],
        raw_out=out,
        scratch=[pltpu.SemaphoreType.DMA((sum(pieces),))],
        flops=flops,
    )


def inverse_rms(values):
    return lax.rsqrt(jnp.mean(values * values, axis=-1, keepdims=True) + NORM_EPS)


def inverse_rms_all(values):
    return lax.rsqrt(jnp.mean(values * values, axis=(0, 1), keepdims=True) + NORM_EPS)


def clamped_unit(gate, linear):
    gate = jnp.minimum(gate, SWIGLU_LIMIT)
    linear = jnp.clip(linear, -SWIGLU_LIMIT, SWIGLU_LIMIT)
    return gate * jax.nn.sigmoid(SWIGLU_ALPHA * gate) * (linear + 1.0)


def peers(size):
    assert size & (size - 1) == 0
    return [[(j, j ^ k) for j in range(size)] for k in range(1, size)]


def swap_all(pieces):
    out = [pieces[0]]
    for k, perm in enumerate(peers(lax.axis_size("tp")), 1):
        out.append(lax.ppermute(pieces[k], "tp", perm))
    return out


def prepare_body(
    keys, cache_values, lengths, tokens, gain, w_forget, bias, gates, routes, logits, after,
    flipped, values, bias_out, hit_out, combine_out, pick_out, tok_out, sems,
):
    del after
    copies = start_copies([cache_values], [values], sems, (2,))
    for s in range(keys.shape[0]):
        flipped[s] = keys[s].T
    seqs, width = tokens.shape
    span = gates.shape[2]
    raw = tokens[...].astype(F32)
    normed = (raw * inverse_rms(raw) * gain[...]).astype(BF16).astype(F32)
    w_rows = w_forget[...].astype(F32)
    lane = lax.broadcasted_iota(jnp.int32, (KVH, span), 1)
    head = lax.broadcasted_iota(jnp.int32, (KVH, 1), 0)
    shift = jnp.zeros((KVH, 1), F32)
    for g in range(KVH):
        shift = jnp.where(head == g, bias[:, g : g + 1], shift)
    for s in range(seqs):
        logit = jnp.sum(normed[s : s + 1] * w_rows, axis=-1, keepdims=True) + shift
        forget = jnp.minimum(logit, 0.0) - jnp.log1p(jnp.exp(-jnp.abs(logit)))
        own_gates = gates[s]
        live = lengths[:, s : s + 1]
        last = jnp.sum(jnp.where(lane == live - 1, own_gates, 0.0), axis=-1, keepdims=True)
        bias_out[s] = jnp.where(lane < live, (last + forget) - own_gates, NEG_LARGE)
        for c in range(width // LANES):
            row = s * (width // LANES) + c
            tok_out[row : row + 1, :] = raw[s : s + 1, c * LANES : (c + 1) * LANES]
    chosen = routes[...]
    scores = logits[...]
    expo = jnp.exp(scores - jnp.max(scores, axis=-1, keepdims=True))
    probs = expo / jnp.sum(expo, axis=-1, keepdims=True)
    expert = lax.broadcasted_iota(jnp.int32, hit_out.shape, 1)
    hit = jnp.zeros(hit_out.shape, F32)
    combine = jnp.zeros(hit_out.shape, F32)
    for k in range(chosen.shape[1]):
        match = (chosen[:, k : k + 1] == expert).astype(F32)
        hit = hit + match
        combine = combine + probs[:, k : k + 1] * match
    pick_out[...] = (chosen[:, :1] == expert).astype(F32)
    hit_out[...] = hit
    combine_out[...] = combine
    for copy in copies:
        copy.wait()


def project_in_body(*refs, groups):
    near, (gain, w_query, w_keyval) = refs[:groups], refs[groups : groups + 3]
    outs, rows = refs[groups + 3 : -1], refs[-1]
    seqs = near[0].shape[0]
    for k in range(groups):
        rows[k * seqs : (k + 1) * seqs, :] = near[k][...].astype(F32)
    raw = rows[...]
    normed = (raw * inverse_rms(raw) * gain[...]).astype(BF16)
    query = jnp.dot(normed, w_query[...], preferred_element_type=F32).astype(BF16)
    pair = jnp.dot(normed, w_keyval[...], preferred_element_type=F32).astype(BF16)
    cols = query.shape[1]
    for k in range(groups):
        outs[k][:, :cols] = query[k * seqs : (k + 1) * seqs]
        outs[k][:, cols:] = pair[k * seqs : (k + 1) * seqs]


def attend_body(*refs, groups, cols):
    near, (keys, values, bias, hit) = refs[:groups], refs[groups : groups + 4]
    mixed_out, fresh_out, pieces, q_rows, mixed_rows = refs[groups + 4 :]
    here = lax.axis_index("tp")
    seqs, _ = near[0].shape
    share = HEADS // KVH
    scale = HDIM ** (-0.5)
    for k in range(groups):
        pieces[here ^ k] = near[k][...].astype(F32)
    fresh = jnp.concatenate([pieces[c][:, cols:] for c in range(groups)], axis=1)
    fresh_out[...] = fresh.astype(BF16)
    q_rows[...] = jnp.zeros(q_rows.shape, F32)
    for s in range(seqs):
        for h in range(HEADS):
            c, at = h * HDIM // cols, h * HDIM % cols
            g = h // share
            q_rows[s * HEADS + h : s * HEADS + h + 1, g * HDIM : (g + 1) * HDIM] = pieces[
                c, s : s + 1, at : at + HDIM
            ]
    head = lax.broadcasted_iota(jnp.int32, (HEADS, 1), 0)
    queries = [q_rows[s * HEADS : (s + 1) * HEADS, :] for s in range(seqs)]
    raws = [jnp.dot(queries[s].astype(BF16), keys[s], preferred_element_type=F32) for s in range(seqs)]
    weights, own_weights = [], []
    for s in range(seqs):
        new_key = fresh[s : s + 1, : KVH * HDIM]
        row_bias = bias[s, KVH - 1 : KVH, :]
        for g in range(KVH - 1):
            row_bias = jnp.where((head >= g * share) & (head < (g + 1) * share), bias[s, g : g + 1, :], row_bias)
        scores = raws[s] * scale + row_bias
        own = jnp.sum(queries[s] * new_key, axis=-1, keepdims=True) * scale
        top = jnp.maximum(jnp.max(scores, axis=-1, keepdims=True), own)
        expo = jnp.exp(scores - top)
        own_expo = jnp.exp(own - top)
        total = 1.0 / (jnp.sum(expo, axis=-1, keepdims=True) + own_expo)
        weights.append((expo * total).astype(BF16))
        own_weights.append((own_expo * total).astype(BF16).astype(F32))
    products = [jnp.dot(weights[s], values[s], preferred_element_type=F32) for s in range(seqs)]
    for s in range(seqs):
        mixed = products[s] + own_weights[s] * fresh[s : s + 1, KVH * HDIM :]
        for h in range(HEADS):
            g = h // share
            mixed_rows[s : s + 1, h * HDIM : (h + 1) * HDIM] = mixed[
                h : h + 1, g * HDIM : (g + 1) * HDIM
            ]
    full = HEADS * HDIM
    mixed_out[:, :full] = mixed_rows[:seqs, :].astype(BF16)
    mixed_out[:, full:] = hit[...].astype(BF16)


def project_out_body(*refs, groups, experts, fold):
    near, tokens, w_out = refs[:groups], refs[groups : 2 * groups], refs[2 * groups]
    out, mixed_rows, parts, hits = refs[2 * groups + 1 :]
    here = lax.axis_index("tp")
    seqs = near[0].shape[0]
    width, cols = w_out.shape
    lanes = cols // fold

    def keep(which, k, rows):
        for s in range(seqs):
            for a in range(fold):
                parts[which * seqs + s, pl.ds(a * groups + (here ^ k), 1), :] = rows[
                    s : s + 1, a * lanes : (a + 1) * lanes
                ]

    for k in range(groups):
        mixed_rows[k * seqs : (k + 1) * seqs, :] = near[k][:, :width].astype(F32)
        hit = near[k][:, width:].astype(F32)
        for s in range(seqs):
            for a in range(fold):
                hits[s, pl.ds(a * groups + (here ^ k), 1), :] = hit[s : s + 1]
        keep(1, k, tokens[k][:, pl.ds(pl.multiple_of(here * cols, LANES), cols)].astype(F32))
    projected = jnp.dot(mixed_rows[...].astype(BF16), w_out[...], preferred_element_type=F32)
    for k in range(groups):
        keep(0, k, projected[k * seqs : (k + 1) * seqs])
    rows = [parts[n] for n in range(2 * seqs)]
    marks = [hits[s] for s in range(seqs)]
    for e in range(experts):
        on = [marks[s][:, e : e + 1] > 0.5 for s in range(seqs)]
        for which in range(2):
            block = jnp.zeros(rows[0].shape, F32)
            for s in range(seqs):
                block = jnp.where(on[s], rows[which * seqs + s], block)
            block = block.astype(BF16)
            for j in range(which, groups, 2):
                out[e * groups + j] = block


def expert_body(
    arrived, other, mix_gain, ffn_gain, w_gate, w_lin, gate_bias, lin_bias, w_down, out, expert_in, answer,
    *, groups, experts, fold
):
    here = lax.axis_index("tp")
    lanes = arrived.shape[1]
    tall = fold * groups
    width = w_gate.shape[0]
    chunks = width // LANES
    side = chunks // groups
    per = lanes // LANES
    blocks, height = out.shape[1:3]
    even = (here & 1) == 0

    def tile(slot, c):
        at = slot * tall
        if not isinstance(slot, int):
            at = pl.multiple_of(at, 8)
        spot = (pl.ds(at, tall), pl.ds(c * LANES, LANES))
        mine, theirs = arrived[spot].astype(F32), other[spot].astype(F32)
        return jnp.where(even, mine, theirs), jnp.where(even, theirs, mine)

    def put(chunk, first, values):
        block, row = chunk // height, chunk % height
        answer[block, pl.ds(first * 8 + row, values.shape[0], stride=8), :] = values

    def close(block):
        for slot in range(groups * experts):
            out[slot, block] = answer[block, slot * 8 : slot * 8 + height, :].astype(BF16)

    if blocks * height > chunks + side:
        answer[...] = jnp.zeros(answer.shape, F32)
    span = max(8 // groups, 1)
    for first in range(0, experts, span):
        near = range(first, first + span)
        projected, tokens = [], []
        for j in range(groups):
            tiles = [[tile(i * groups + j, c) for i in near] for c in range(per)]
            for a in range(fold):
                for c in range(per):
                    rows = [
                        [pair[n][a * groups : (a + 1) * groups] for pair in tiles[c]] for n in range(2)
                    ]
                    projected.append(jnp.concatenate(rows[0], axis=0))
                    tokens.append(jnp.concatenate(rows[1], axis=0))
        projected = jnp.concatenate(projected, axis=1)
        tokens = jnp.concatenate(tokens, axis=1)
        residual = tokens + projected * inverse_rms(projected) * mix_gain[...]
        normed = residual * inverse_rms(residual) * ffn_gain[...]
        at, count = first * groups, span * groups
        expert_in[at : at + count, :] = normed.astype(BF16)
        for c in range(per):
            tiles = [tile(i * groups + here, c)[0] for i in near]
            for a in range(fold):
                mine = jnp.concatenate([t[a * groups : (a + 1) * groups] for t in tiles], axis=0)
                put(chunks + a * per + c, at, mine)
    rows = expert_in[...]
    hidden = w_gate.shape[1]
    cut = hidden // 2 if hidden % (4 * LANES) == 0 else hidden
    acts = []
    for at in range(0, hidden, cut):
        span = slice(at, at + cut)
        gate = jnp.dot(rows, w_gate[:, span], preferred_element_type=F32) + gate_bias[:, span]
        linear = jnp.dot(rows, w_lin[:, span], preferred_element_type=F32) + lin_bias[:, span]
        acts.append(clamped_unit(gate, linear).astype(BF16))
    act = jnp.concatenate(acts, axis=1)
    for block in range(chunks // height, blocks):
        close(block)
    wide = height * LANES
    for block in range(chunks // height):
        part = jnp.dot(
            act, w_down[:, block * wide : (block + 1) * wide], preferred_element_type=F32
        )
        for c in range(height):
            put(block * height + c, 0, part[:, c * LANES : (c + 1) * LANES])
        close(block)


def finish_body(
    returned, tokens, combine, pick, mix_gain, post_gain, out, rows, moe, near, *, groups, experts
):
    seqs, width = out.shape
    chunks = width // LANES
    side = chunks // groups
    height = returned.shape[2]
    tall = chunks // height
    zero = jnp.zeros((height, LANES), F32)
    sums = [[zero] * tall for _ in range(seqs)]
    own = [[zero] * groups for _ in range(seqs)]
    for e in range(experts):
        picked = [jnp.broadcast_to(pick[s : s + 1, e : e + 1], zero.shape) for s in range(seqs)]
        shares = [jnp.broadcast_to(combine[s : s + 1, e : e + 1], zero.shape) for s in range(seqs)]
        for b in range(tall):
            total = zero
            for j in range(groups):
                total = total + returned[e * groups + j, b].astype(F32)
            total = total.astype(BF16).astype(F32)
            for s in range(seqs):
                sums[s][b] = sums[s][b] + shares[s] * total
        for j in range(groups):
            part = returned[e * groups + j, tall].astype(F32)
            for s in range(seqs):
                own[s][j] = own[s][j] + picked[s] * part
    for s in range(seqs):
        for b in range(tall):
            moe[b * height : (b + 1) * height, :] = sums[s][b]
        for j in range(groups):
            near[j * side : (j + 1) * side, :] = own[s][j][:side]
        projected, mixture = near[...], moe[...]
        residual = (
            tokens[s * chunks : (s + 1) * chunks, :]
            + projected * inverse_rms_all(projected) * mix_gain[...]
        )
        updated = residual + mixture * inverse_rms_all(mixture) * post_gain[...]
        for c in range(chunks):
            rows[s : s + 1, c * LANES : (c + 1) * LANES] = updated[c : c + 1, :]
    out[...] = rows[:seqs, :].astype(BF16)


def layer(
    tokens,
    cache_keys,
    cache_values,
    cache_gates,
    lengths,
    routes,
    route_logits,
    attn_gain,
    w_query,
    w_keyval,
    w_forget,
    forget_bias,
    w_out,
    mix_gain,
    ffn_gain,
    w_gate,
    w_lin,
    gate_bias,
    lin_bias,
    w_down,
    post_gain,
):
    groups = lax.axis_size("tp")
    experts = lax.axis_size("ep")
    both_axes = ("ep", "tp")
    seqs, width = tokens.shape
    span = cache_keys.shape[1]
    cols = w_query.shape[1]
    pair = w_keyval.shape[1]
    chunks = width // LANES
    slots = experts * groups
    out_cols = w_out.shape[1]
    fold = 2 if groups < 8 and out_cols % (2 * LANES) == 0 else 1
    marked = -(-experts // LANES) * LANES
    row = lambda gain: gain.reshape(1, width)
    block = lambda gain: gain.reshape(chunks, LANES)

    near_tokens = swap_all([tokens] * groups)
    w_query, w_keyval, keys = load([w_query, w_keyval, cache_keys], (2, 1, 2), LOAD_FLOPS)
    sent = call(
        functools.partial(project_in_body, groups=groups),
        [((seqs, cols + pair), BF16)] * groups,
        [*near_tokens, row(attn_gain), w_query, w_keyval],
        scratch=[((groups * seqs, width), F32)],
    )
    near = swap_all(sent)
    keys, values, bias, hit, combine, pick, own_tokens = call(
        prepare_body,
        [
            ((seqs, KVH * HDIM, span), BF16),
            (cache_values.shape, BF16),
            ((seqs, KVH, span), F32),
            ((seqs, marked), F32),
            ((seqs, marked), F32),
            ((seqs, marked), F32),
            ((seqs * chunks, LANES), F32),
        ],
        [
            keys,
            cache_values,
            lengths.reshape(1, seqs),
            tokens,
            row(attn_gain),
            w_forget.T,
            forget_bias.reshape(1, KVH),
            cache_gates,
            routes,
            route_logits,
            sent[0],
        ],
        hbm=(1,),
        scratch=[pltpu.SemaphoreType.DMA((2,))],
        flops=LOAD_FLOPS,
    )
    mixed, fresh = call(
        functools.partial(attend_body, groups=groups, cols=cols),
        [((seqs, width + marked), BF16), ((seqs, 2 * KVH * HDIM), BF16)],
        [*near, keys, values, bias, hit],
        scratch=[
            ((groups, seqs, cols + pair), F32),
            ((seqs * HEADS, KVH * HDIM), F32),
            ((max(seqs, 8), HEADS * HDIM), F32),
        ],
    )
    near_mixed = swap_all([mixed] * groups)
    w_out, fresh = load([w_out, fresh], (2, 1), LOAD_FLOPS, [mixed], out=(1,))
    (outbound,) = call(
        functools.partial(project_out_body, groups=groups, experts=experts, fold=fold),
        [((slots, fold * groups, out_cols // fold), BF16)],
        [*near_mixed, *near_tokens, w_out],
        scratch=[
            ((groups * seqs, width), F32),
            ((2 * seqs, fold * groups, out_cols // fold), F32),
            ((seqs, fold * groups, marked), F32),
        ],
    )
    arrived = lax.all_to_all(outbound, both_axes, 0, 0, tiled=True)
    arrived = arrived.reshape(slots * fold * groups, out_cols // fold)
    other = lax.ppermute(arrived, "tp", [(j, j ^ 1) for j in range(groups)])
    used = chunks + chunks // groups
    height = 4 if 1 <= used % 8 <= 4 else 8
    blocks = -(-used // height)
    (answers,) = call(
        functools.partial(expert_body, groups=groups, experts=experts, fold=fold),
        [((slots, blocks, height, LANES), BF16)],
        [
            arrived,
            other,
            row(mix_gain),
            row(ffn_gain),
            w_gate[0],
            w_lin[0],
            gate_bias,
            lin_bias,
            w_down[0],
        ],
        scratch=[
            ((slots, width), BF16),
            ((blocks, slots * 8, LANES), F32),
        ],
    )
    returned = lax.all_to_all(answers, both_axes, 0, 0, tiled=True)
    (updated,) = call(
        functools.partial(finish_body, groups=groups, experts=experts),
        [((seqs, width), BF16)],
        [returned, own_tokens, combine, pick, block(mix_gain), block(post_gain)],
        hbm_out=(0,),
        scratch=[
            ((max(seqs, 8), width), F32),
            ((chunks, LANES), F32),
            ((chunks, LANES), F32),
        ],
    )
    return (updated, fresh)


def solution(mesh):
    in_specs = (
        P(("ep", "tp"), None),
        P(("ep", "tp"), None, None),
        P(("ep", "tp"), None, None),
        P(("ep", "tp"), None, None),
        P(("ep", "tp")),
        P(("ep", "tp"), None),
        P(("ep", "tp"), None),
        P(),
        P(None, "tp"),
        P(None, "tp"),
        P(),
        P(),
        P(None, "tp"),
        P(),
        P(),
        P("ep", None, "tp"),
        P("ep", None, "tp"),
        P("ep", "tp"),
        P("ep", "tp"),
        P("ep", "tp", None),
        P(),
    )
    out_specs = (P(("ep", "tp"), None), P(("ep", "tp"), None))
    return jax.shard_map(layer, mesh=mesh, in_specs=in_specs, out_specs=out_specs, check_vma=False)
```

```python
import functools
import math

import jax
import jax.numpy as jnp
from jax import lax
from jax.experimental import pallas as pl
from jax.experimental.pallas import tpu as pltpu
from jax.sharding import Mesh
from jax.sharding import PartitionSpec as P


TP = ("chip", "core")
CORES = 2
HEADS = 16
KVH = 2
HDIM = 128
LANES = 128

NORM_EPS = 1e-06
SWIGLU_ALPHA = 1.702
SWIGLU_LIMIT = 7.0
NEG_LARGE = -1e30

LOAD_FLOPS = 50_000_000


F32 = jnp.float32
BF16 = jnp.bfloat16
VMEM = pltpu.VMEM
SMEM = pltpu.SMEM


def call(body, outs, args, smem=(), hbm=(), hbm_out=(), raw_out=(), scratch=(), flops=0):
    spaces = [
        SMEM if i in smem else pl.ANY if i in hbm else VMEM for i in range(len(args))
    ]
    args = [
        pltpu.with_memory_space_constraint(a, VMEM)
        if space is VMEM
        else pltpu.with_memory_space_constraint(a, pltpu.HBM)
        if space is pl.ANY
        else a
        for a, space in zip(args, spaces)
    ]
    room = 4 << 20
    for entry in scratch:
        if isinstance(entry, tuple):
            room += 2 * math.prod(entry[0]) * jnp.dtype(entry[1]).itemsize
    return pl.pallas_call(
        body,
        out_shape=[
            jax.ShapeDtypeStruct(shape, dtype) if i in (*hbm_out, *raw_out) else VMEM(shape, dtype)
            for i, (shape, dtype) in enumerate(outs)
        ],
        in_specs=[pl.BlockSpec(memory_space=space) for space in spaces],
        out_specs=[
            pl.BlockSpec(memory_space=pl.ANY if i in raw_out else VMEM) for i in range(len(outs))
        ],
        scratch_shapes=[
            VMEM(*entry) if isinstance(entry, tuple) else entry for entry in scratch
        ],
        compiler_params=pltpu.CompilerParams(vmem_limit_bytes=room),
        cost_estimate=pl.CostEstimate(flops=flops, transcendentals=0, bytes_accessed=0),
    )(*args)


def start_copies(sources, targets, sems, pieces):
    copies = []
    for source, target, cuts in zip(sources, targets, pieces):
        size = source.shape[0] // cuts
        for c in range(cuts):
            part = pl.ds(c * size, size)
            copies.append(
                pltpu.make_async_copy(source.at[part], target.at[part], sems.at[len(copies)])
            )
    for copy in copies:
        copy.start()
    return copies


def load_body(*refs, pieces):
    count = len(pieces)
    for copy in start_copies(refs[:count], refs[-count - 1 : -1], refs[-1], pieces):
        copy.wait()


def load(arrays, pieces, flops, after=(), out=()):
    return call(
        functools.partial(load_body, pieces=pieces),
        [(a.shape, a.dtype) for a in arrays],
        [*arrays, *after],
        hbm=[i for i in range(len(arrays)) if i not in out],
        raw_out=out,
        scratch=[pltpu.SemaphoreType.DMA((sum(pieces),))],
        flops=flops,
    )


def inverse_rms(values):
    return lax.rsqrt(jnp.mean(values * values, axis=-1, keepdims=True) + NORM_EPS)


def inverse_rms_all(values):
    return lax.rsqrt(jnp.mean(values * values, axis=(0, 1), keepdims=True) + NORM_EPS)


def clamped_unit(gate, linear):
    gate = jnp.minimum(gate, SWIGLU_LIMIT)
    linear = jnp.clip(linear, -SWIGLU_LIMIT, SWIGLU_LIMIT)
    return gate * jax.nn.sigmoid(SWIGLU_ALPHA * gate) * (linear + 1.0)


def peers(size):
    assert size & (size - 1) == 0
    return [[(j, j ^ k) for j in range(size)] for k in range(1, size)]


def swap_all(pieces):
    out = [pieces[0]]
    for k, perm in enumerate(peers(lax.axis_size(TP)), 1):
        out.append(lax.ppermute(pieces[k], TP, perm))
    return out


def prepare_body(
    keys, cache_values, lengths, tokens, gain, w_forget, bias, gates, routes, logits, after,
    flipped, values, bias_out, hit_out, combine_out, pick_out, tok_out, sems,
):
    del after
    copies = start_copies([cache_values], [values], sems, (2,))
    for s in range(keys.shape[0]):
        flipped[s] = keys[s].T
    seqs, width = tokens.shape
    span = gates.shape[2]
    raw = tokens[...].astype(F32)
    normed = (raw * inverse_rms(raw) * gain[...]).astype(BF16).astype(F32)
    w_rows = w_forget[...].astype(F32)
    lane = lax.broadcasted_iota(jnp.int32, (KVH, span), 1)
    head = lax.broadcasted_iota(jnp.int32, (KVH, 1), 0)
    shift = jnp.zeros((KVH, 1), F32)
    for g in range(KVH):
        shift = jnp.where(head == g, bias[:, g : g + 1], shift)
    for s in range(seqs):
        logit = jnp.sum(normed[s : s + 1] * w_rows, axis=-1, keepdims=True) + shift
        forget = jnp.minimum(logit, 0.0) - jnp.log1p(jnp.exp(-jnp.abs(logit)))
        own_gates = gates[s]
        live = lengths[:, s : s + 1]
        last = jnp.sum(jnp.where(lane == live - 1, own_gates, 0.0), axis=-1, keepdims=True)
        bias_out[s] = jnp.where(lane < live, (last + forget) - own_gates, NEG_LARGE)
        for c in range(width // LANES):
            row = s * (width // LANES) + c
            tok_out[row : row + 1, :] = raw[s : s + 1, c * LANES : (c + 1) * LANES]
    chosen = routes[...]
    scores = logits[...]
    expo = jnp.exp(scores - jnp.max(scores, axis=-1, keepdims=True))
    probs = expo / jnp.sum(expo, axis=-1, keepdims=True)
    expert = lax.broadcasted_iota(jnp.int32, hit_out.shape, 1)
    hit = jnp.zeros(hit_out.shape, F32)
    combine = jnp.zeros(hit_out.shape, F32)
    for k in range(chosen.shape[1]):
        match = (chosen[:, k : k + 1] == expert).astype(F32)
        hit = hit + match
        combine = combine + probs[:, k : k + 1] * match
    pick_out[...] = (chosen[:, :1] == expert).astype(F32)
    hit_out[...] = hit
    combine_out[...] = combine
    for copy in copies:
        copy.wait()


def project_in_body(*refs, groups, edge):
    near, (gain, w_query, w_keyval, *biases) = refs[:groups], refs[groups : groups + 5]
    outs, rows = refs[groups + 5 : -1], refs[-1]
    hidden = biases[0].shape[1]
    for n, bias in enumerate(biases):
        whole = bias[...]
        high = whole.astype(BF16)
        outs[1][n : n + 1, edge : edge + hidden] = high
        outs[1][n : n + 1, edge + hidden :] = (whole - high.astype(F32)).astype(BF16)
    seqs = near[0].shape[0]
    for k in range(groups):
        rows[k * seqs : (k + 1) * seqs, :] = near[k][...].astype(F32)
    raw = rows[...]
    normed = (raw * inverse_rms(raw) * gain[...]).astype(BF16)
    query = jnp.dot(normed, w_query[...], preferred_element_type=F32).astype(BF16)
    pair = jnp.dot(normed, w_keyval[...], preferred_element_type=F32).astype(BF16)
    cols = query.shape[1]
    for k in range(groups):
        outs[k][:, :cols] = query[k * seqs : (k + 1) * seqs]
        outs[k][:, cols : cols + pair.shape[1]] = pair[k * seqs : (k + 1) * seqs]


def attend_body(*refs, groups, cols):
    near, (keys, values, bias, hit) = refs[:groups], refs[groups : groups + 4]
    mixed_out, fresh_out, pieces, q_rows, mixed_rows = refs[groups + 4 :]
    here = lax.axis_index("chip") * CORES + lax.axis_index("core")
    seqs, width = near[0].shape
    share = HEADS // KVH
    scale = HDIM ** (-0.5)
    for k in range(groups):
        pieces[here ^ k] = near[k][:, :width].astype(F32)
    fresh = jnp.concatenate([pieces[c][:, cols:] for c in range(groups)], axis=1)
    fresh_out[...] = fresh.astype(BF16)
    q_rows[...] = jnp.zeros(q_rows.shape, F32)
    for s in range(seqs):
        for h in range(HEADS):
            c, at = h * HDIM // cols, h * HDIM % cols
            g = h // share
            q_rows[s * HEADS + h : s * HEADS + h + 1, g * HDIM : (g + 1) * HDIM] = pieces[
                c, s : s + 1, at : at + HDIM
            ]
    head = lax.broadcasted_iota(jnp.int32, (HEADS, 1), 0)
    queries = [q_rows[s * HEADS : (s + 1) * HEADS, :] for s in range(seqs)]
    raws = [jnp.dot(queries[s].astype(BF16), keys[s], preferred_element_type=F32) for s in range(seqs)]
    weights, own_weights = [], []
    for s in range(seqs):
        new_key = fresh[s : s + 1, : KVH * HDIM]
        row_bias = bias[s, KVH - 1 : KVH, :]
        for g in range(KVH - 1):
            row_bias = jnp.where((head >= g * share) & (head < (g + 1) * share), bias[s, g : g + 1, :], row_bias)
        scores = raws[s] * scale + row_bias
        own = jnp.sum(queries[s] * new_key, axis=-1, keepdims=True) * scale
        top = jnp.maximum(jnp.max(scores, axis=-1, keepdims=True), own)
        expo = jnp.exp(scores - top)
        own_expo = jnp.exp(own - top)
        total = 1.0 / (jnp.sum(expo, axis=-1, keepdims=True) + own_expo)
        weights.append((expo * total).astype(BF16))
        own_weights.append((own_expo * total).astype(BF16).astype(F32))
    products = [jnp.dot(weights[s], values[s], preferred_element_type=F32) for s in range(seqs)]
    for s in range(seqs):
        mixed = products[s] + own_weights[s] * fresh[s : s + 1, KVH * HDIM :]
        for h in range(HEADS):
            g = h // share
            mixed_rows[s : s + 1, h * HDIM : (h + 1) * HDIM] = mixed[
                h : h + 1, g * HDIM : (g + 1) * HDIM
            ]
    full = HEADS * HDIM
    mixed_out[:, :full] = mixed_rows[:seqs, :].astype(BF16)
    mixed_out[:, full:] = hit[...].astype(BF16)


def project_out_body(*refs, groups, experts, fold):
    near, tokens, w_out = refs[:groups], refs[groups : 2 * groups], refs[2 * groups]
    out, mixed_rows, parts, hits = refs[2 * groups + 1 :]
    here = lax.axis_index("chip") * CORES + lax.axis_index("core")
    seqs = near[0].shape[0]
    width, cols = w_out.shape
    lanes = cols // fold
    chips = groups // CORES

    def keep(which, k, rows):
        core, chip = (here ^ k) & 1, (here ^ k) >> 1
        for s in range(seqs):
            for a in range(fold):
                parts[core * seqs + s, pl.ds((which * fold + a) * chips + chip, 1), :] = rows[
                    s : s + 1, a * lanes : (a + 1) * lanes
                ]

    for k in range(groups):
        mixed_rows[k * seqs : (k + 1) * seqs, :] = near[k][:, :width].astype(F32)
        hit = near[k][:, width:].astype(F32)
        core, chip = (here ^ k) & 1, (here ^ k) >> 1
        for s in range(seqs):
            for n in range(2 * fold):
                hits[core * seqs + s, pl.ds(n * chips + chip, 1), :] = hit[s : s + 1]
        keep(1, k, tokens[k][:, pl.ds(pl.multiple_of(here * cols, LANES), cols)].astype(F32))
    projected = jnp.dot(mixed_rows[...].astype(BF16), w_out[...], preferred_element_type=F32)
    for k in range(groups):
        keep(0, k, projected[k * seqs : (k + 1) * seqs])
    rows = [parts[n] for n in range(CORES * seqs)]
    marks = [hits[n] for n in range(CORES * seqs)]
    for e in range(experts):
        for core in range(CORES):
            block = jnp.zeros(rows[0].shape, F32)
            for s in range(seqs):
                n = core * seqs + s
                block = jnp.where(marks[n][:, e : e + 1] > 0.5, rows[n], block)
            block = block.astype(BF16)
            for chip in range(chips):
                out[e * groups + chip * CORES + core] = block


def expert_body(
    arrived, mix_gain, ffn_gain, w_gate, w_lin, gate_bias, lin_bias, w_down, gate_by, lin_by, down_by, biases_by, out, expert_in, answer,
    *, groups, experts, fold, edge
):
    lanes = arrived.shape[1]
    tall = fold * groups
    width = w_gate.shape[0]
    chunks = width // LANES
    chips = groups // CORES
    side = chunks // chips
    per = lanes // LANES
    slots = experts * chips
    blocks, height = out.shape[1:3]
    across = lax.axis_index("chip")

    def tile(slot, c):
        return arrived[pl.ds(slot * tall, tall), c * LANES : (c + 1) * LANES].astype(F32)

    def put(chunk, first, values):
        block, row = chunk // height, chunk % height
        answer[block, pl.ds(first * 8 + row, values.shape[0], stride=8), :] = values

    def close(block):
        for slot in range(slots):
            out[slot, block] = answer[block, slot * 8 : slot * 8 + height, :].astype(BF16)

    if blocks * height > chunks + side:
        answer[...] = jnp.zeros(answer.shape, F32)
    span = max(8 // chips, 1)
    for first in range(0, experts, span):
        near = range(first, first + span)
        both = [[], []]
        for j in range(groups):
            tiles = [[tile(i * groups + j, c) for i in near] for c in range(per)]
            for which in range(2):
                for a in range(fold):
                    at = (which * fold + a) * chips
                    for c in range(per):
                        both[which].append(
                            jnp.concatenate([t[at : at + chips] for t in tiles[c]], axis=0)
                        )
        projected, tokens = (jnp.concatenate(parts, axis=1) for parts in both)
        residual = tokens + projected * inverse_rms(projected) * mix_gain[...]
        normed = residual * inverse_rms(residual) * ffn_gain[...]
        at, count = first * chips, span * chips
        expert_in[at : at + count, :] = normed.astype(BF16)
        mine = jnp.zeros((count, side * LANES), F32)
        for chip in range(chips):
            piece = projected[:, chip * side * LANES : (chip + 1) * side * LANES]
            mine = jnp.where(across == chip, piece, mine)
        for c in range(side):
            put(chunks + c, at, mine[:, c * LANES : (c + 1) * LANES])
    rows = expert_in[...]
    acts = []
    hidden = w_gate.shape[1]
    parts = biases_by[:2, edge:].astype(F32)
    shifts = parts[:, :hidden] + parts[:, hidden:]
    for gate_w, lin_w, gate_shift, lin_shift in (
        (w_gate, w_lin, gate_bias[...], lin_bias[...]),
        (gate_by, lin_by, shifts[0:1], shifts[1:2]),
    ):
        gate = jnp.dot(rows, gate_w[...], preferred_element_type=F32) + gate_shift
        linear = jnp.dot(rows, lin_w[...], preferred_element_type=F32) + lin_shift
        acts.append(clamped_unit(gate, linear).astype(BF16))
    for block in range(chunks // height, blocks):
        close(block)
    wide = height * LANES
    for block in range(chunks // height):
        span = slice(block * wide, (block + 1) * wide)
        part = jnp.dot(acts[0], w_down[:, span], preferred_element_type=F32)
        part = part + jnp.dot(acts[1], down_by[:, span], preferred_element_type=F32)
        for c in range(height):
            put(block * height + c, 0, part[:, c * LANES : (c + 1) * LANES])
        close(block)


def finish_body(
    returned, tokens, combine, pick, mix_gain, post_gain, out, rows, moe, near, *, chips, experts
):
    seqs, width = out.shape
    chunks = width // LANES
    side = chunks // chips
    height = returned.shape[2]
    tall = chunks // height
    wings = -(-side // height)
    zero = jnp.zeros((height, LANES), F32)
    sums = [[zero] * tall for _ in range(seqs)]
    own = [[[zero] * wings for _ in range(chips)] for _ in range(seqs)]
    for e in range(experts):
        picked = [jnp.broadcast_to(pick[s : s + 1, e : e + 1], zero.shape) for s in range(seqs)]
        shares = [jnp.broadcast_to(combine[s : s + 1, e : e + 1], zero.shape) for s in range(seqs)]
        for b in range(tall):
            total = zero
            for j in range(chips):
                total = total + returned[e * chips + j, b].astype(F32)
            total = total.astype(BF16).astype(F32)
            for s in range(seqs):
                sums[s][b] = sums[s][b] + shares[s] * total
        for j in range(chips):
            for b in range(wings):
                part = returned[e * chips + j, tall + b].astype(F32)
                for s in range(seqs):
                    own[s][j][b] = own[s][j][b] + picked[s] * part
    for s in range(seqs):
        for b in range(tall):
            moe[b * height : (b + 1) * height, :] = sums[s][b]
        for j in range(chips):
            for b in range(wings):
                count = min(height, side - b * height)
                at = j * side + b * height
                near[at : at + count, :] = own[s][j][b][:count]
        projected, mixture = near[...], moe[...]
        residual = (
            tokens[s * chunks : (s + 1) * chunks, :]
            + projected * inverse_rms_all(projected) * mix_gain[...]
        )
        updated = residual + mixture * inverse_rms_all(mixture) * post_gain[...]
        for c in range(chunks):
            rows[s : s + 1, c * LANES : (c + 1) * LANES] = updated[c : c + 1, :]
    out[...] = rows[:seqs, :].astype(BF16)


def layer(
    tokens,
    cache_keys,
    cache_values,
    cache_gates,
    lengths,
    routes,
    route_logits,
    attn_gain,
    w_query,
    w_keyval,
    w_forget,
    forget_bias,
    w_out,
    mix_gain,
    ffn_gain,
    w_gate,
    w_lin,
    gate_bias,
    lin_bias,
    w_down,
    post_gain,
):
    groups = lax.axis_size(TP)
    experts = lax.axis_size("ep")
    both_axes = ("ep", *TP)
    seqs, width = tokens.shape
    span = cache_keys.shape[1]
    cols = w_query.shape[1]
    pair = w_keyval.shape[1]
    chunks = width // LANES
    edge = -(-(cols + pair) // LANES) * LANES
    slots = experts * groups
    chips = groups // CORES
    out_cols = w_out.shape[1]
    fold = 2 if groups < 8 and out_cols % (2 * LANES) == 0 else 1
    marked = -(-experts // LANES) * LANES
    row = lambda gain: gain.reshape(1, width)
    block = lambda gain: gain.reshape(chunks, LANES)

    near_tokens = swap_all([tokens] * groups)
    w_query, w_keyval, keys = load([w_query, w_keyval, cache_keys], (2, 1, 2), LOAD_FLOPS)
    sent = call(
        functools.partial(project_in_body, groups=groups, edge=edge),
        [
            ((seqs, edge + 2 * gate_bias.shape[1] if k == 1 else cols + pair), BF16)
            for k in range(groups)
        ],
        [*near_tokens, row(attn_gain), w_query, w_keyval, gate_bias, lin_bias],
        scratch=[((groups * seqs, width), F32)],
    )
    near = swap_all(sent)
    by = []
    for array in (w_gate[0], w_lin[0], w_down[0]):
        by.append(lax.ppermute(array, "core", [(0, 1), (1, 0)]))
    keys, values, bias, hit, combine, pick, own_tokens = call(
        prepare_body,
        [
            ((seqs, KVH * HDIM, span), BF16),
            (cache_values.shape, BF16),
            ((seqs, KVH, span), F32),
            ((seqs, marked), F32),
            ((seqs, marked), F32),
            ((seqs, marked), F32),
            ((seqs * chunks, LANES), F32),
        ],
        [
            keys,
            cache_values,
            lengths.reshape(1, seqs),
            tokens,
            row(attn_gain),
            w_forget.T,
            forget_bias.reshape(1, KVH),
            cache_gates,
            routes,
            route_logits,
            sent[0],
        ],
        hbm=(1,),
        scratch=[pltpu.SemaphoreType.DMA((2,))],
        flops=LOAD_FLOPS,
    )
    mixed, fresh = call(
        functools.partial(attend_body, groups=groups, cols=cols),
        [((seqs, width + marked), BF16), ((seqs, 2 * KVH * HDIM), BF16)],
        [*near, keys, values, bias, hit],
        scratch=[
            ((groups, seqs, cols + pair), F32),
            ((seqs * HEADS, KVH * HDIM), F32),
            ((max(seqs, 8), HEADS * HDIM), F32),
        ],
    )
    near_mixed = swap_all([mixed] * groups)
    w_out, fresh = load([w_out, fresh], (2, 1), LOAD_FLOPS, [mixed], out=(1,))
    (outbound,) = call(
        functools.partial(project_out_body, groups=groups, experts=experts, fold=fold),
        [((slots, fold * groups, out_cols // fold), BF16)],
        [*near_mixed, *near_tokens, w_out],
        scratch=[
            ((groups * seqs, width), F32),
            ((2 * seqs, fold * groups, out_cols // fold), F32),
            ((2 * seqs, fold * groups, marked), F32),
        ],
    )
    arrived = lax.all_to_all(outbound, both_axes, 0, 0, tiled=True)
    arrived = arrived.reshape(slots * fold * groups, out_cols // fold)
    used = chunks + chunks // chips
    height = 4 if 1 <= used % 8 <= 4 else 8
    blocks = -(-used // height)
    (answers,) = call(
        functools.partial(expert_body, groups=groups, experts=experts, fold=fold, edge=edge),
        [((experts * chips, blocks, height, LANES), BF16)],
        [
            arrived,
            row(mix_gain),
            row(ffn_gain),
            w_gate[0],
            w_lin[0],
            gate_bias,
            lin_bias,
            w_down[0],
            *by,
            near[1],
        ],
        scratch=[
            ((experts * chips, width), BF16),
            ((blocks, experts * chips * 8, LANES), F32),
        ],
    )
    returned = lax.all_to_all(answers, ("ep", "chip"), 0, 0, tiled=True)
    (updated,) = call(
        functools.partial(finish_body, chips=chips, experts=experts),
        [((seqs, width), BF16)],
        [returned, own_tokens, combine, pick, block(mix_gain), block(post_gain)],
        hbm_out=(0,),
        scratch=[
            ((max(seqs, 8), width), F32),
            ((chunks, LANES), F32),
            ((chunks, LANES), F32),
        ],
    )
    return (updated, fresh)


def solution(mesh):
    groups = mesh.shape["tp"]
    split = Mesh(mesh.devices.reshape(-1, groups // CORES, CORES), ("ep", *TP))
    in_specs = (
        P(("ep", *TP), None),
        P(("ep", *TP), None, None),
        P(("ep", *TP), None, None),
        P(("ep", *TP), None, None),
        P(("ep", *TP)),
        P(("ep", *TP), None),
        P(("ep", *TP), None),
        P(),
        P(None, TP),
        P(None, TP),
        P(),
        P(),
        P(None, TP),
        P(),
        P(),
        P("ep", None, TP),
        P("ep", None, TP),
        P("ep", TP),
        P("ep", TP),
        P("ep", TP, None),
        P(),
    )
    out_specs = (P(("ep", *TP), None), P(("ep", *TP), None))
    return jax.shard_map(layer, mesh=split, in_specs=in_specs, out_specs=out_specs, check_vma=False)
```

```python
import functools
import math

import jax
import jax.numpy as jnp
from jax import lax
from jax.experimental import pallas as pl
from jax.experimental.pallas import tpu as pltpu
from jax.sharding import Mesh
from jax.sharding import PartitionSpec as P


TP = ("chip", "core")
CORES = 2
HEADS = 16
KVH = 2
HDIM = 128
LANES = 128

NORM_EPS = 1e-06
SWIGLU_ALPHA = 1.702
SWIGLU_LIMIT = 7.0
NEG_LARGE = -1e30

LOAD_FLOPS = 50_000_000


F32 = jnp.float32
BF16 = jnp.bfloat16
VMEM = pltpu.VMEM
SMEM = pltpu.SMEM


def call(body, outs, args, smem=(), hbm=(), hbm_out=(), raw_out=(), scratch=(), flops=0):
    spaces = [
        SMEM if i in smem else pl.ANY if i in hbm else VMEM for i in range(len(args))
    ]
    args = [
        pltpu.with_memory_space_constraint(a, VMEM)
        if space is VMEM
        else pltpu.with_memory_space_constraint(a, pltpu.HBM)
        if space is pl.ANY
        else a
        for a, space in zip(args, spaces)
    ]
    room = 4 << 20
    for entry in scratch:
        if isinstance(entry, tuple):
            room += 2 * math.prod(entry[0]) * jnp.dtype(entry[1]).itemsize
    return pl.pallas_call(
        body,
        out_shape=[
            jax.ShapeDtypeStruct(shape, dtype) if i in (*hbm_out, *raw_out) else VMEM(shape, dtype)
            for i, (shape, dtype) in enumerate(outs)
        ],
        in_specs=[pl.BlockSpec(memory_space=space) for space in spaces],
        out_specs=[
            pl.BlockSpec(memory_space=pl.ANY if i in raw_out else VMEM) for i in range(len(outs))
        ],
        scratch_shapes=[
            VMEM(*entry) if isinstance(entry, tuple) else entry for entry in scratch
        ],
        compiler_params=pltpu.CompilerParams(vmem_limit_bytes=room),
        cost_estimate=pl.CostEstimate(flops=flops, transcendentals=0, bytes_accessed=0),
    )(*args)


def start_copies(sources, targets, sems, pieces):
    copies = []
    for source, target, cuts in zip(sources, targets, pieces):
        size = source.shape[0] // cuts
        for c in range(cuts):
            part = pl.ds(c * size, size)
            copies.append(
                pltpu.make_async_copy(source.at[part], target.at[part], sems.at[len(copies)])
            )
    for copy in copies:
        copy.start()
    return copies


def load_body(*refs, pieces):
    count = len(pieces)
    for copy in start_copies(refs[:count], refs[-count - 1 : -1], refs[-1], pieces):
        copy.wait()


def load(arrays, pieces, flops, after=(), out=()):
    return call(
        functools.partial(load_body, pieces=pieces),
        [(a.shape, a.dtype) for a in arrays],
        [*arrays, *after],
        hbm=[i for i in range(len(arrays)) if i not in out],
        raw_out=out,
        scratch=[pltpu.SemaphoreType.DMA((sum(pieces),))],
        flops=flops,
    )


def inverse_rms(values):
    return lax.rsqrt(jnp.mean(values * values, axis=-1, keepdims=True) + NORM_EPS)


def inverse_rms_all(values):
    return lax.rsqrt(jnp.mean(values * values, axis=(0, 1), keepdims=True) + NORM_EPS)


def clamped_unit(gate, linear):
    gate = jnp.minimum(gate, SWIGLU_LIMIT)
    linear = jnp.clip(linear, -SWIGLU_LIMIT, SWIGLU_LIMIT)
    return gate * jax.nn.sigmoid(SWIGLU_ALPHA * gate) * (linear + 1.0)


def peers(size):
    assert size & (size - 1) == 0
    return [[(j, j ^ k) for j in range(size)] for k in range(1, size)]


def swap_all(pieces):
    out = [pieces[0]]
    for k, perm in enumerate(peers(lax.axis_size(TP)), 1):
        out.append(lax.ppermute(pieces[k], TP, perm))
    return out


def prepare_body(
    cache_keys, cache_values, lengths, tokens, gain, w_forget, bias, gates, routes, logits, after,
    flipped, values, bias_out, hit_out, combine_out, pick_out, tok_out, keys, sems,
):
    del after
    cuts = (keys.shape[0], 1)
    copies = start_copies([cache_keys, cache_values], [keys, values], sems, cuts)
    seqs, width = tokens.shape
    span = gates.shape[2]
    raw = tokens[...].astype(F32)
    normed = (raw * inverse_rms(raw) * gain[...]).astype(BF16).astype(F32)
    w_rows = w_forget[...].astype(F32)
    lane = lax.broadcasted_iota(jnp.int32, (KVH, span), 1)
    head = lax.broadcasted_iota(jnp.int32, (KVH, 1), 0)
    shift = jnp.zeros((KVH, 1), F32)
    for g in range(KVH):
        shift = jnp.where(head == g, bias[:, g : g + 1], shift)
    for s in range(seqs):
        logit = jnp.sum(normed[s : s + 1] * w_rows, axis=-1, keepdims=True) + shift
        forget = jnp.minimum(logit, 0.0) - jnp.log1p(jnp.exp(-jnp.abs(logit)))
        own_gates = gates[s]
        live = lengths[:, s : s + 1]
        last = jnp.sum(jnp.where(lane == live - 1, own_gates, 0.0), axis=-1, keepdims=True)
        bias_out[s] = jnp.where(lane < live, (last + forget) - own_gates, NEG_LARGE)
        for c in range(width // LANES):
            row = s * (width // LANES) + c
            tok_out[row : row + 1, :] = raw[s : s + 1, c * LANES : (c + 1) * LANES]
    chosen = routes[...]
    scores = logits[...]
    expo = jnp.exp(scores - jnp.max(scores, axis=-1, keepdims=True))
    probs = expo / jnp.sum(expo, axis=-1, keepdims=True)
    expert = lax.broadcasted_iota(jnp.int32, hit_out.shape, 1)
    hit = jnp.zeros(hit_out.shape, F32)
    combine = jnp.zeros(hit_out.shape, F32)
    for k in range(chosen.shape[1]):
        match = (chosen[:, k : k + 1] == expert).astype(F32)
        hit = hit + match
        combine = combine + probs[:, k : k + 1] * match
    pick_out[...] = (chosen[:, :1] == expert).astype(F32)
    hit_out[...] = hit
    combine_out[...] = combine
    for s in range(seqs):
        copies[s].wait()
        flipped[s] = keys[s].T
    for copy in copies[seqs:]:
        copy.wait()


def project_in_body(*refs, groups, edge):
    near, (gain, w_query, w_keyval, *biases) = refs[:groups], refs[groups : groups + 5]
    outs, rows = refs[groups + 5 : -1], refs[-1]
    hidden = biases[0].shape[1]
    for n, bias in enumerate(biases):
        whole = bias[...]
        high = whole.astype(BF16)
        outs[1][n : n + 1, edge : edge + hidden] = high
        outs[1][n : n + 1, edge + hidden :] = (whole - high.astype(F32)).astype(BF16)
    seqs = near[0].shape[0]
    for k in range(groups):
        rows[k * seqs : (k + 1) * seqs, :] = near[k][...].astype(F32)
    raw = rows[...]
    normed = (raw * inverse_rms(raw) * gain[...]).astype(BF16)
    query = jnp.dot(normed, w_query[...], preferred_element_type=F32).astype(BF16)
    pair = jnp.dot(normed, w_keyval[...], preferred_element_type=F32).astype(BF16)
    cols = query.shape[1]
    for k in range(groups):
        outs[k][:, :cols] = query[k * seqs : (k + 1) * seqs]
        outs[k][:, cols : cols + pair.shape[1]] = pair[k * seqs : (k + 1) * seqs]


def attend_body(*refs, groups, cols):
    near, (keys, values, bias, hit) = refs[:groups], refs[groups : groups + 4]
    mixed_out, fresh_out, pieces, q_rows, mixed_rows = refs[groups + 4 :]
    here = lax.axis_index("chip") * CORES + lax.axis_index("core")
    seqs, width = near[0].shape
    share = HEADS // KVH
    scale = HDIM ** (-0.5)
    for k in range(groups):
        pieces[here ^ k] = near[k][:, :width].astype(F32)
    fresh = jnp.concatenate([pieces[c][:, cols:] for c in range(groups)], axis=1)
    fresh_out[...] = fresh.astype(BF16)
    q_rows[...] = jnp.zeros(q_rows.shape, F32)
    for s in range(seqs):
        for h in range(HEADS):
            c, at = h * HDIM // cols, h * HDIM % cols
            g = h // share
            q_rows[s * HEADS + h : s * HEADS + h + 1, g * HDIM : (g + 1) * HDIM] = pieces[
                c, s : s + 1, at : at + HDIM
            ]
    head = lax.broadcasted_iota(jnp.int32, (HEADS, 1), 0)
    queries = [q_rows[s * HEADS : (s + 1) * HEADS, :] for s in range(seqs)]
    raws = [jnp.dot(queries[s].astype(BF16), keys[s], preferred_element_type=F32) for s in range(seqs)]
    weights, own_weights = [], []
    for s in range(seqs):
        new_key = fresh[s : s + 1, : KVH * HDIM]
        row_bias = bias[s, KVH - 1 : KVH, :]
        for g in range(KVH - 1):
            row_bias = jnp.where((head >= g * share) & (head < (g + 1) * share), bias[s, g : g + 1, :], row_bias)
        scores = raws[s] * scale + row_bias
        own = jnp.sum(queries[s] * new_key, axis=-1, keepdims=True) * scale
        top = jnp.maximum(jnp.max(scores, axis=-1, keepdims=True), own)
        expo = jnp.exp(scores - top)
        own_expo = jnp.exp(own - top)
        total = 1.0 / (jnp.sum(expo, axis=-1, keepdims=True) + own_expo)
        weights.append((expo * total).astype(BF16))
        own_weights.append((own_expo * total).astype(BF16).astype(F32))
    products = [jnp.dot(weights[s], values[s], preferred_element_type=F32) for s in range(seqs)]
    for s in range(seqs):
        mixed = products[s] + own_weights[s] * fresh[s : s + 1, KVH * HDIM :]
        for h in range(HEADS):
            g = h // share
            mixed_rows[s : s + 1, h * HDIM : (h + 1) * HDIM] = mixed[
                h : h + 1, g * HDIM : (g + 1) * HDIM
            ]
    full = HEADS * HDIM
    mixed_out[:, :full] = mixed_rows[:seqs, :].astype(BF16)
    mixed_out[:, full:] = hit[...].astype(BF16)


def project_out_body(*refs, groups, experts, fold):
    near, tokens, w_out = refs[:groups], refs[groups : 2 * groups], refs[2 * groups]
    out, mixed_rows, parts, hits = refs[2 * groups + 1 :]
    here = lax.axis_index("chip") * CORES + lax.axis_index("core")
    seqs = near[0].shape[0]
    width, cols = w_out.shape
    lanes = cols // fold
    chips = groups // CORES

    def keep(which, k, rows):
        core, chip = (here ^ k) & 1, (here ^ k) >> 1
        for s in range(seqs):
            for a in range(fold):
                parts[core * seqs + s, pl.ds((which * fold + a) * chips + chip, 1), :] = rows[
                    s : s + 1, a * lanes : (a + 1) * lanes
                ]

    for k in range(groups):
        mixed_rows[k * seqs : (k + 1) * seqs, :] = near[k][:, :width].astype(F32)
        hit = near[k][:, width:].astype(F32)
        core, chip = (here ^ k) & 1, (here ^ k) >> 1
        for s in range(seqs):
            for n in range(2 * fold):
                hits[core * seqs + s, pl.ds(n * chips + chip, 1), :] = hit[s : s + 1]
        keep(1, k, tokens[k][:, pl.ds(pl.multiple_of(here * cols, LANES), cols)].astype(F32))
    projected = jnp.dot(mixed_rows[...].astype(BF16), w_out[...], preferred_element_type=F32)
    for k in range(groups):
        keep(0, k, projected[k * seqs : (k + 1) * seqs])
    rows = [parts[n] for n in range(CORES * seqs)]
    marks = [hits[n] for n in range(CORES * seqs)]
    for e in range(experts):
        for core in range(CORES):
            block = jnp.zeros(rows[0].shape, F32)
            for s in range(seqs):
                n = core * seqs + s
                block = jnp.where(marks[n][:, e : e + 1] > 0.5, rows[n], block)
            block = block.astype(BF16)
            for chip in range(chips):
                out[e * groups + chip * CORES + core] = block


def expert_body(
    arrived, mix_gain, ffn_gain, w_gate, w_lin, gate_bias, lin_bias, w_down, gate_by, lin_by, down_by, biases_by, out, expert_in, answer,
    *, groups, experts, fold, edge
):
    lanes = arrived.shape[1]
    tall = fold * groups
    width = w_gate.shape[0]
    chunks = width // LANES
    chips = groups // CORES
    side = chunks // chips
    per = lanes // LANES
    slots = experts * chips
    blocks, height = out.shape[1:3]
    across = lax.axis_index("chip")

    def tile(slot, c):
        return arrived[pl.ds(slot * tall, tall), c * LANES : (c + 1) * LANES].astype(F32)

    def put(chunk, first, values):
        block, row = chunk // height, chunk % height
        answer[block, pl.ds(first * 8 + row, values.shape[0], stride=8), :] = values

    def close(block):
        for slot in range(slots):
            out[slot, block] = answer[block, slot * 8 : slot * 8 + height, :].astype(BF16)

    if blocks * height > chunks + side:
        answer[...] = jnp.zeros(answer.shape, F32)
    span = max(8 // chips, 1)
    for first in range(0, experts, span):
        near = range(first, first + span)
        both = [[], []]
        for j in range(groups):
            tiles = [[tile(i * groups + j, c) for i in near] for c in range(per)]
            for which in range(2):
                for a in range(fold):
                    at = (which * fold + a) * chips
                    for c in range(per):
                        both[which].append(
                            jnp.concatenate([t[at : at + chips] for t in tiles[c]], axis=0)
                        )
        projected, tokens = (jnp.concatenate(parts, axis=1) for parts in both)
        residual = tokens + projected * inverse_rms(projected) * mix_gain[...]
        normed = residual * inverse_rms(residual) * ffn_gain[...]
        at, count = first * chips, span * chips
        expert_in[at : at + count, :] = normed.astype(BF16)
        mine = jnp.zeros((count, side * LANES), F32)
        for chip in range(chips):
            piece = projected[:, chip * side * LANES : (chip + 1) * side * LANES]
            mine = jnp.where(across == chip, piece, mine)
        for c in range(side):
            put(chunks + c, at, mine[:, c * LANES : (c + 1) * LANES])
    rows = expert_in[...]
    acts = []
    hidden = w_gate.shape[1]
    parts = biases_by[:2, edge:].astype(F32)
    shifts = parts[:, :hidden] + parts[:, hidden:]
    for gate_w, lin_w, gate_shift, lin_shift in (
        (w_gate, w_lin, gate_bias[...], lin_bias[...]),
        (gate_by, lin_by, shifts[0:1], shifts[1:2]),
    ):
        gate = jnp.dot(rows, gate_w[...], preferred_element_type=F32) + gate_shift
        linear = jnp.dot(rows, lin_w[...], preferred_element_type=F32) + lin_shift
        acts.append(clamped_unit(gate, linear).astype(BF16))
    for block in range(chunks // height, blocks):
        close(block)
    wide = height * LANES
    for block in range(chunks // height):
        span = slice(block * wide, (block + 1) * wide)
        part = jnp.dot(acts[0], w_down[:, span], preferred_element_type=F32)
        part = part + jnp.dot(acts[1], down_by[:, span], preferred_element_type=F32)
        for c in range(height):
            put(block * height + c, 0, part[:, c * LANES : (c + 1) * LANES])
        close(block)


def finish_body(
    returned, tokens, combine, pick, mix_gain, post_gain, out, rows, moe, near, *, chips, experts
):
    seqs, width = out.shape
    chunks = width // LANES
    side = chunks // chips
    height = returned.shape[2]
    tall = chunks // height
    wings = -(-side // height)
    zero = jnp.zeros((height, LANES), F32)
    sums = [[zero] * tall for _ in range(seqs)]
    own = [[[zero] * wings for _ in range(chips)] for _ in range(seqs)]
    for e in range(experts):
        picked = [jnp.broadcast_to(pick[s : s + 1, e : e + 1], zero.shape) for s in range(seqs)]
        shares = [jnp.broadcast_to(combine[s : s + 1, e : e + 1], zero.shape) for s in range(seqs)]
        for b in range(tall):
            total = zero
            for j in range(chips):
                total = total + returned[e * chips + j, b].astype(F32)
            total = total.astype(BF16).astype(F32)
            for s in range(seqs):
                sums[s][b] = sums[s][b] + shares[s] * total
        for j in range(chips):
            for b in range(wings):
                part = returned[e * chips + j, tall + b].astype(F32)
                for s in range(seqs):
                    own[s][j][b] = own[s][j][b] + picked[s] * part
    for s in range(seqs):
        for b in range(tall):
            moe[b * height : (b + 1) * height, :] = sums[s][b]
        for j in range(chips):
            for b in range(wings):
                count = min(height, side - b * height)
                at = j * side + b * height
                near[at : at + count, :] = own[s][j][b][:count]
        projected, mixture = near[...], moe[...]
        residual = (
            tokens[s * chunks : (s + 1) * chunks, :]
            + projected * inverse_rms_all(projected) * mix_gain[...]
        )
        updated = residual + mixture * inverse_rms_all(mixture) * post_gain[...]
        for c in range(chunks):
            rows[s : s + 1, c * LANES : (c + 1) * LANES] = updated[c : c + 1, :]
    out[...] = rows[:seqs, :].astype(BF16)


def layer(
    tokens,
    cache_keys,
    cache_values,
    cache_gates,
    lengths,
    routes,
    route_logits,
    attn_gain,
    w_query,
    w_keyval,
    w_forget,
    forget_bias,
    w_out,
    mix_gain,
    ffn_gain,
    w_gate,
    w_lin,
    gate_bias,
    lin_bias,
    w_down,
    post_gain,
):
    groups = lax.axis_size(TP)
    experts = lax.axis_size("ep")
    both_axes = ("ep", *TP)
    seqs, width = tokens.shape
    span = cache_keys.shape[1]
    cols = w_query.shape[1]
    pair = w_keyval.shape[1]
    chunks = width // LANES
    edge = -(-(cols + pair) // LANES) * LANES
    slots = experts * groups
    chips = groups // CORES
    out_cols = w_out.shape[1]
    fold = 2 if groups < 8 and out_cols % (2 * LANES) == 0 else 1
    marked = -(-experts // LANES) * LANES
    row = lambda gain: gain.reshape(1, width)
    block = lambda gain: gain.reshape(chunks, LANES)

    near_tokens = swap_all([tokens] * groups)
    w_query, w_keyval = load([w_query, w_keyval], (2, 1), LOAD_FLOPS)
    sent = call(
        functools.partial(project_in_body, groups=groups, edge=edge),
        [
            ((seqs, edge + 2 * gate_bias.shape[1] if k == 1 else cols + pair), BF16)
            for k in range(groups)
        ],
        [*near_tokens, row(attn_gain), w_query, w_keyval, gate_bias, lin_bias],
        scratch=[((groups * seqs, width), F32)],
    )
    near = swap_all(sent)
    by = []
    for array in (w_gate[0], w_lin[0], w_down[0]):
        by.append(lax.ppermute(array, "core", [(0, 1), (1, 0)]))
    keys, values, bias, hit, combine, pick, own_tokens = call(
        prepare_body,
        [
            ((seqs, KVH * HDIM, span), BF16),
            (cache_values.shape, BF16),
            ((seqs, KVH, span), F32),
            ((seqs, marked), F32),
            ((seqs, marked), F32),
            ((seqs, marked), F32),
            ((seqs * chunks, LANES), F32),
        ],
        [
            cache_keys,
            cache_values,
            lengths.reshape(1, seqs),
            tokens,
            row(attn_gain),
            w_forget.T,
            forget_bias.reshape(1, KVH),
            cache_gates,
            routes,
            route_logits,
            sent[0],
        ],
        hbm=(0, 1),
        scratch=[(cache_keys.shape, BF16), pltpu.SemaphoreType.DMA((seqs + 1,))],
        flops=LOAD_FLOPS,
    )
    mixed, fresh = call(
        functools.partial(attend_body, groups=groups, cols=cols),
        [((seqs, width + marked), BF16), ((seqs, 2 * KVH * HDIM), BF16)],
        [*near, keys, values, bias, hit],
        scratch=[
            ((groups, seqs, cols + pair), F32),
            ((seqs * HEADS, KVH * HDIM), F32),
            ((max(seqs, 8), HEADS * HDIM), F32),
        ],
    )
    near_mixed = swap_all([mixed] * groups)
    w_out, fresh = load([w_out, fresh], (2, 1), LOAD_FLOPS, [mixed], out=(1,))
    (outbound,) = call(
        functools.partial(project_out_body, groups=groups, experts=experts, fold=fold),
        [((slots, fold * groups, out_cols // fold), BF16)],
        [*near_mixed, *near_tokens, w_out],
        scratch=[
            ((groups * seqs, width), F32),
            ((2 * seqs, fold * groups, out_cols // fold), F32),
            ((2 * seqs, fold * groups, marked), F32),
        ],
    )
    arrived = lax.all_to_all(outbound, both_axes, 0, 0, tiled=True)
    arrived = arrived.reshape(slots * fold * groups, out_cols // fold)
    used = chunks + chunks // chips
    height = 4 if 1 <= used % 8 <= 4 else 8
    blocks = -(-used // height)
    (answers,) = call(
        functools.partial(expert_body, groups=groups, experts=experts, fold=fold, edge=edge),
        [((experts * chips, blocks, height, LANES), BF16)],
        [
            arrived,
            row(mix_gain),
            row(ffn_gain),
            w_gate[0],
            w_lin[0],
            gate_bias,
            lin_bias,
            w_down[0],
            *by,
            near[1],
        ],
        scratch=[
            ((experts * chips, width), BF16),
            ((blocks, experts * chips * 8, LANES), F32),
        ],
    )
    returned = lax.all_to_all(answers, ("ep", "chip"), 0, 0, tiled=True)
    (updated,) = call(
        functools.partial(finish_body, chips=chips, experts=experts),
        [((seqs, width), BF16)],
        [returned, own_tokens, combine, pick, block(mix_gain), block(post_gain)],
        hbm_out=(0,),
        scratch=[
            ((max(seqs, 8), width), F32),
            ((chunks, LANES), F32),
            ((chunks, LANES), F32),
        ],
    )
    return (updated, fresh)


def solution(mesh):
    groups = mesh.shape["tp"]
    split = Mesh(mesh.devices.reshape(-1, groups // CORES, CORES), ("ep", *TP))
    in_specs = (
        P(("ep", *TP), None),
        P(("ep", *TP), None, None),
        P(("ep", *TP), None, None),
        P(("ep", *TP), None, None),
        P(("ep", *TP)),
        P(("ep", *TP), None),
        P(("ep", *TP), None),
        P(),
        P(None, TP),
        P(None, TP),
        P(),
        P(),
        P(None, TP),
        P(),
        P(),
        P("ep", None, TP),
        P("ep", None, TP),
        P("ep", TP),
        P("ep", TP),
        P("ep", TP, None),
        P(),
    )
    out_specs = (P(("ep", *TP), None), P(("ep", *TP), None))
    return jax.shard_map(layer, mesh=split, in_specs=in_specs, out_specs=out_specs, check_vma=False)
```
